256 devices in a mesh: st: 64 (over z, y, core), tp: 4 (over x).
Axes of the slice: x: 4, y: 4, z: 8, core: 2. Of those that a mesh axis runs over, the one named last changes fastest.
Arguments:
- tokens: bfloat16 [24576, 2048], P('st', 'tp'), may hold values from -6 to 6
- cotangent: bfloat16 [24576, 1024], P('st', 'tp'), may hold values from -48 to 48
- mix_query: bfloat16 [24576, 1024], P('st', 'tp'), may hold values from -6 to 6
- mix_key: bfloat16 [24576, 1024], P('st', 'tp'), may hold values from -6 to 6
- mix_value: bfloat16 [24576, 1024], P('st', 'tp'), may hold values from -24 to 24
- beta_pre: float32 [8, 24576], P('tp', 'st'), may hold values from -9 to 9
- decay_pre: float32 [8, 24576], P('tp', 'st'), may hold values from -8 to 6
- decay_rate: float32 [8], P('tp'), may hold values from 0.001 to 0.06
- passages: bfloat16 [1024, 64, 2048], P('st'), may hold values from -16 to 16
- passage_ids: int32 [384, 4], P('st'), may hold values from 0 to 1023, as said below
- query_weight: bfloat16 [2048, 1024], P(None, 'tp'), may hold values from -0.125 to 0.125
- key_weight: bfloat16 [2048, 1024], P(None, 'tp'), may hold values from -0.125 to 0.125
- value_weight: bfloat16 [2048, 1024], P(None, 'tp'), may hold values from -0.125 to 0.125
- gate_weight: bfloat16 [4, 2048], P('tp'), may hold values from -0.125 to 0.125
Outputs:
- token_grad: bfloat16 [24576, 2048], P('st', 'tp')
- passage_grad: bfloat16 [1024, 64, 2048], P('st', None, 'tp')
- key_weight_grad: float32 [2048, 1024], P('st', 'tp')
The draws below stay inside these ranges and needn't reach their ends.
Inputs may be any that keep to these rules, and one draw needn't show every extreme that they name: Passage p is stored on index p // 16 of st. The rows of passage_ids read by one index of st name at most 1 passages stored on any one index of st, and exactly 1 on some.
All inputs are finite; a program needn't handle non-finite values.
Results may differ from the reference program's by a relative error of at most 0.012.
The reference program's roundings to bfloat16 on the way count: a program that leaves them out, or rounds other values in their place, can miss the bound.
Values may be sent and summed in bfloat16 or wider, within the bound.
No kernel may reach another device: no remote copies, remote signals or barrier semaphores. Data moves between devices by JAX's collectives and lax.ppermute only.
A program may use at most 128 MiB of HBM per device.

```python
import math
import jax
import jax.numpy as jnp
from jax import lax

D = 2048
HEADS = 4
HEAD = 256
MIX_HEADS = 8
MIX_DIM = 128
SPAN = 64
BLOCK = 64
PER_BLOCK = 4
PROWS = 64
TOK_DEV = 384
PASS_DEV = 16
TOKENS = 24576
BLOCKS = 384
REQ_DEV = 24
CAP = 1
PASSAGES = 1024
N_ST = 64


def draw_passage_ids(key, part):
    slot_count = N_ST * CAP
    shift_table = jax.random.randint(jax.random.fold_in(key, 9001), (N_ST,), 0, PASS_DEV)

    def per_reader(reader_idx):
        keys_split = jax.random.split(jax.random.fold_in(key, reader_idx), 4)
        rank_score = jax.random.permutation(keys_split[0], slot_count).astype(jnp.int32)
        slot_owner = jnp.arange(slot_count, dtype=jnp.int32) // CAP
        forced = (slot_owner == (reader_idx - 1) % N_ST) | (slot_owner == (reader_idx + N_ST // 2) % N_ST)
        rank_score = rank_score + forced.astype(jnp.int32) * (2 * slot_count)
        _, chosen = lax.top_k(rank_score, REQ_DEV)
        chosen = chosen.astype(jnp.int32)[jax.random.permutation(keys_split[1], REQ_DEV)]
        owner_ids = chosen // CAP
        first_draw = jax.random.randint(keys_split[2], (REQ_DEV,), 0, PASS_DEV)
        second_draw = jax.random.randint(keys_split[3], (REQ_DEV,), 0, PASS_DEV)
        local_ids = (jnp.minimum(first_draw, second_draw) + shift_table[owner_ids]) % PASS_DEV
        return (owner_ids * PASS_DEV + local_ids).astype(jnp.int32)
    every_id = jax.vmap(per_reader)(jnp.arange(N_ST, dtype=jnp.int32))
    return every_id.reshape(BLOCKS, PER_BLOCK)


def draw_decay_pre(key, part):
    keys_split = jax.random.split(key, 3)
    noise_part = 0.7 * jax.random.normal(keys_split[0], (MIX_HEADS, TOKENS), jnp.float32)
    slow_part = jax.random.uniform(keys_split[1], (MIX_HEADS, TOKENS // SPAN), jnp.float32, -1.2, 1.2)
    device_part = jax.random.uniform(keys_split[2], (MIX_HEADS, N_ST), jnp.float32, -1.0, 1.0)
    values_out = noise_part + jnp.repeat(slow_part, SPAN, axis=1) + jnp.repeat(device_part, TOK_DEV, axis=1)
    return jnp.clip(values_out, -8.0, 6.0)


def spiked(array, rng, source, target, parts, factor):
    owner, partner = [(jnp.arange(array.shape[dim]) // (array.shape[dim] // parts)).reshape([-1 if axis == dim else 1 for axis in range(array.ndim)]) for dim in (source, target)]
    chosen = jax.random.permutation(rng, parts)[partner]
    strong = (owner == chosen) | (owner == (partner + parts // 2) % parts)
    return jnp.where(strong, factor * array, array)


def level_of(key, extent, cuts, low, largest):
    def one(axis_at, blocks):
        draws = jax.random.uniform(jax.random.fold_in(jax.random.fold_in(key, 6), axis_at), (blocks,), jnp.float32, low / len(cuts), largest / len(cuts))
        return jnp.repeat(jnp.exp(draws), extent[axis_at] // blocks).reshape((-1,) + (1,) * (len(extent) - axis_at - 1))

    level = one(*cuts[0])
    for cut in cuts[1:]:
        level = level * one(*cut)
    return level


def scatter_about(rng, shape, scale, reach, pieces=(), kind=jnp.bfloat16):
    loudness = level_of(rng, shape, pieces, -0.22, 0.18) if pieces else 1.0
    values = jax.random.normal(rng, shape, jnp.float32) * scale * loudness
    return jnp.minimum(jnp.maximum(values, -reach), reach).astype(kind)


def noise_with(rng, extent, deviation, most, cuts, heavy, kind=jnp.bfloat16):
    entries = deviation * jax.random.normal(rng, extent, jnp.float32)
    if cuts:
        entries = entries * level_of(rng, extent, cuts, -0.22, 0.18)
    return jnp.clip(spiked(entries, jax.random.fold_in(rng, 3), *heavy), -most, most).astype(kind)


def setup_inputs(seed: int = 0) -> dict:
    streams_of = jax.random.split(jax.random.key(seed), 15)
    tokens = scatter_about(streams_of[0], (TOKENS, D), 1.0, 6.0, ((0, 64), (1, 4)))
    cotangent = scatter_about(streams_of[1], (TOKENS, HEADS * HEAD), 8.0, 48.0, ((0, 64), (1, 4)))
    mix_query = scatter_about(streams_of[2], (TOKENS, MIX_HEADS * MIX_DIM), 1.0, 6.0, ((0, 64), (1, 4)))
    mix_key = scatter_about(streams_of[3], (TOKENS, MIX_HEADS * MIX_DIM), 1.0, 6.0, ((0, 64), (1, 4)))
    mix_value = scatter_about(streams_of[4], (TOKENS, MIX_HEADS * MIX_DIM), 4.0, 24.0, ((0, 64), (1, 4)))
    beta_pre = scatter_about(streams_of[5], (MIX_HEADS, TOKENS), 1.5, 9.0, ((0, 4), (1, 64)), jnp.float32)
    decay_pre = draw_decay_pre(jax.random.fold_in(streams_of[14], 71), 0)
    decay_rate = jnp.clip(jnp.exp(math.log(0.06) - 4.0943445 * jax.random.uniform(streams_of[7], (MIX_HEADS,), jnp.float32) ** level_of(streams_of[7], (MIX_HEADS,), ((0, 4),), -0.2, 0.2)), 0.001, 0.06)
    passages = noise_with(streams_of[8], (PASSAGES, PROWS, D), 1.0, 16.0, ((0, 64),), (0, 2, 64, 4.0))
    passage_ids = draw_passage_ids(jax.random.fold_in(streams_of[14], 71), 0)
    query_weight = scatter_about(streams_of[10], (D, HEADS * HEAD), D ** -0.5, 0.125, ((1, 4),))
    key_weight = scatter_about(streams_of[11], (D, HEADS * HEAD), D ** -0.5, 0.125, ((1, 4),))
    value_weight = scatter_about(streams_of[12], (D, HEADS * HEAD), D ** -0.5, 0.125, ((1, 4),))
    gate_weight = scatter_about(streams_of[13], (HEADS, D), D ** -0.5, 0.125, ((0, 4),))
    return dict(tokens=tokens, cotangent=cotangent, mix_query=mix_query, mix_key=mix_key, mix_value=mix_value, beta_pre=beta_pre, decay_pre=decay_pre, decay_rate=decay_rate, passages=passages, passage_ids=passage_ids, query_weight=query_weight, key_weight=key_weight, value_weight=value_weight, gate_weight=gate_weight)


NORM_FLOOR = 1.0
SCORE_GAIN = 4.0
HIGHEST = lax.Precision.HIGHEST

def to_low(value):
    return lax.optimization_barrier(value.astype(jnp.bfloat16))

def neumann_inverse(strict_part):
    span_size = strict_part.shape[-1]
    unit_eye = jnp.eye(span_size, dtype=jnp.float32)
    running = unit_eye - strict_part
    power_term = strict_part
    for _ in range(span_size.bit_length() - 2):
        power_term = jnp.einsum('...ij,...jk->...ik', power_term, power_term, precision=HIGHEST)
        running = jnp.einsum('...ij,...jk->...ik', running, unit_eye + power_term, precision=HIGHEST)
    return running

def delta_mixer(queries, keys_in, values_in, strength, log_decay):
    heads_n, length, key_dim = queries.shape
    blocks_n = length // SPAN

    def to_blocks(tensor):
        return tensor.reshape(heads_n, blocks_n, SPAN, *tensor.shape[2:])
    queries, keys_in, values_in = (to_blocks(queries), to_blocks(keys_in), to_blocks(values_in))
    strength, log_decay = (to_blocks(strength), to_blocks(log_decay))
    cumulative = jnp.cumsum(log_decay, axis=-1)
    position = jnp.arange(SPAN)
    inclusive = position[:, None] >= position[None, :]
    strictly = position[:, None] > position[None, :]
    spread = jnp.where(inclusive, cumulative[..., :, None] - cumulative[..., None, :], -jnp.inf)
    decay_map = jnp.exp(spread)
    key_gram = jnp.einsum('hncd,hnmd->hncm', keys_in, keys_in, precision=HIGHEST)
    strict_part = jnp.where(strictly, strength[..., :, None] * key_gram * decay_map, 0.0)
    inverse = neumann_inverse(strict_part)
    fresh_vals = jnp.einsum('hncm,hnme->hnce', inverse, values_in * strength[..., None], precision=HIGHEST)
    correction = jnp.einsum('hncm,hnmd->hncd', inverse, keys_in * (strength * jnp.exp(cumulative))[..., None], precision=HIGHEST)
    attend_map = jnp.where(inclusive, jnp.einsum('hncd,hnmd->hncm', queries, keys_in, precision=HIGHEST) * decay_map, 0.0)
    query_dec = queries * jnp.exp(cumulative)[..., None]
    key_dec = keys_in * jnp.exp(cumulative[..., -1:] - cumulative)[..., None]
    carry_decay = jnp.exp(cumulative[..., -1])

    def advance(memory_state, inputs):
        fresh_blk, correct_blk, attend_blk, query_blk, key_blk, decay_blk = inputs
        new_values = fresh_blk - jnp.einsum('hcd,hde->hce', correct_blk, memory_state, precision=HIGHEST)
        output = jnp.einsum('hcd,hde->hce', query_blk, memory_state, precision=HIGHEST) + jnp.einsum('hcm,hme->hce', attend_blk, new_values, precision=HIGHEST)
        memory_state = memory_state * decay_blk[:, None, None] + jnp.einsum('hcd,hce->hde', key_blk, new_values, precision=HIGHEST)
        return (memory_state, output)
    stacked = tuple((jnp.moveaxis(tensor, 1, 0) for tensor in (fresh_vals, correction, attend_map, query_dec, key_dec, carry_decay)))
    initial = jnp.zeros((heads_n, key_dim, values_in.shape[-1]), jnp.float32)
    _, outputs = lax.scan(advance, initial, stacked)
    return jnp.transpose(outputs, (1, 0, 2, 3)).reshape(heads_n, length, -1)

def mixer_output(query_raw, key_raw, value_raw, beta_raw, decay_raw, rate_vals):
    length = query_raw.shape[0]
    heads_n = beta_raw.shape[0]

    def heads_first(matrix):
        return jnp.transpose(matrix.astype(jnp.float32).reshape(length, heads_n, -1), (1, 0, 2))
    queries = heads_first(query_raw)
    keys_in = heads_first(key_raw)
    values_in = heads_first(value_raw)
    queries = queries * lax.rsqrt(lax.optimization_barrier(jnp.sum(queries * queries, axis=-1, keepdims=True)) + NORM_FLOOR) * queries.shape[-1] ** (-0.5)
    keys_in = keys_in * lax.rsqrt(lax.optimization_barrier(jnp.sum(keys_in * keys_in, axis=-1, keepdims=True)) + NORM_FLOOR)
    strength = jax.nn.sigmoid(beta_raw)
    log_decay = -rate_vals[:, None] * jax.nn.softplus(decay_raw)
    mixer_out = delta_mixer(queries, keys_in, values_in, strength, log_decay)
    return jnp.transpose(mixer_out, (1, 0, 2)).reshape(length, -1)

def request_slots(id_rows, pass_count):
    owners = id_rows // pass_count
    local_idx = id_rows % pass_count
    req_count = id_rows.shape[-1]
    req_order = jnp.arange(req_count, dtype=jnp.int32)
    earlier = (owners[..., :, None] == owners[..., None, :]) & (req_order[None, :] < req_order[:, None])
    ranks = lax.optimization_barrier(jnp.sum(earlier.astype(jnp.int32), axis=-1, dtype=jnp.int32))
    return (owners, local_idx, ranks)

def reference(tokens, cotangent, mix_query, mix_key, mix_value, beta_pre, decay_pre, decay_rate, passages, passage_ids, query_weight, key_weight, value_weight, gate_weight):
    score_scale = SCORE_GAIN * HEAD ** (-0.5)
    every_id = passage_ids.reshape(N_ST, REQ_DEV)
    query_heads = query_weight.astype(jnp.float32).reshape(D, HEADS, HEAD)
    key_heads = key_weight.astype(jnp.float32).reshape(D, HEADS, HEAD)
    value_heads = value_weight.astype(jnp.float32).reshape(D, HEADS, HEAD)
    gate_float = gate_weight.astype(jnp.float32)
    blocks_n = TOK_DEV // BLOCK

    def reader(reader_idx):
        first_row = reader_idx * TOK_DEV
        tok_block = lax.dynamic_slice_in_dim(tokens, first_row, TOK_DEV, 0)
        query_low = to_low(jnp.dot(tok_block, query_weight, preferred_element_type=jnp.float32))
        query_float = query_low.astype(jnp.float32).reshape(TOK_DEV, HEADS, HEAD)
        query_scale = lax.rsqrt(lax.optimization_barrier(jnp.mean(query_float * query_float, axis=-1, keepdims=True)) + NORM_FLOOR)
        query_hat = to_low(query_float * query_scale)
        gate_open = jax.nn.sigmoid(jnp.dot(tok_block, gate_weight.T, preferred_element_type=jnp.float32))
        row_block = passages[every_id[reader_idx]].reshape(REQ_DEV * PROWS, D)
        key_low = to_low(jnp.dot(row_block, key_weight, preferred_element_type=jnp.float32))
        key_float = key_low.astype(jnp.float32).reshape(REQ_DEV * PROWS, HEADS, HEAD)
        key_scale = lax.rsqrt(lax.optimization_barrier(jnp.mean(key_float * key_float, axis=-1, keepdims=True)) + NORM_FLOOR)
        key_hat = to_low(key_float * key_scale)
        value_low = to_low(jnp.dot(row_block, value_weight, preferred_element_type=jnp.float32))
        key_blocks = key_hat.astype(jnp.float32).reshape(blocks_n, PER_BLOCK * PROWS, HEADS, HEAD)
        value_blocks = value_low.astype(jnp.float32).reshape(blocks_n, PER_BLOCK * PROWS, HEADS, HEAD)
        query_blocks = query_hat.astype(jnp.float32).reshape(blocks_n, BLOCK, HEADS, HEAD)
        scores = jnp.einsum('bihd,bjhd->bhij', query_blocks, key_blocks) * score_scale
        exp_scores = jnp.exp(scores)
        attn_probs = exp_scores / lax.optimization_barrier(jnp.sum(exp_scores, axis=-1, keepdims=True))
        probs_low = to_low(attn_probs).astype(jnp.float32)
        retrieved = jnp.einsum('bhij,bjhd->bihd', probs_low, value_blocks).reshape(TOK_DEV, HEADS, HEAD)
        mixer_out = mixer_output(lax.dynamic_slice_in_dim(mix_query, first_row, TOK_DEV, 0), lax.dynamic_slice_in_dim(mix_key, first_row, TOK_DEV, 0), lax.dynamic_slice_in_dim(mix_value, first_row, TOK_DEV, 0), lax.dynamic_slice_in_dim(beta_pre, first_row, TOK_DEV, 1), lax.dynamic_slice_in_dim(decay_pre, first_row, TOK_DEV, 1), decay_rate).reshape(TOK_DEV, HEADS, HEAD)
        grad_out = lax.dynamic_slice_in_dim(cotangent, first_row, TOK_DEV, 0).astype(jnp.float32).reshape(TOK_DEV, HEADS, HEAD)
        grad_ret = to_low(gate_open[..., None] * grad_out).astype(jnp.float32)
        gate_grad = lax.optimization_barrier(jnp.sum(grad_out * (retrieved - mixer_out), axis=-1)) * gate_open * (1.0 - gate_open)
        grad_blocks = grad_ret.reshape(blocks_n, BLOCK, HEADS, HEAD)
        grad_probs = jnp.einsum('bihd,bjhd->bhij', grad_blocks, value_blocks)
        score_grad = to_low(attn_probs * (grad_probs - lax.optimization_barrier(jnp.sum(grad_probs * attn_probs, axis=-1, keepdims=True)))).astype(jnp.float32)
        qhat_grad = score_scale * jnp.einsum('bhij,bjhd->bihd', score_grad, key_blocks).reshape(TOK_DEV, HEADS, HEAD)
        khat_grad = to_low(score_scale * jnp.einsum('bhij,bihd->bjhd', score_grad, query_blocks)).astype(jnp.float32).reshape(REQ_DEV, PROWS, HEADS, HEAD)
        value_grad = to_low(jnp.einsum('bhij,bihd->bjhd', probs_low, grad_blocks)).astype(jnp.float32).reshape(REQ_DEV, PROWS, HEADS, HEAD)
        query_grad = to_low(query_scale * qhat_grad - query_scale ** 3 * query_float * lax.optimization_barrier(jnp.mean(query_float * qhat_grad, axis=-1, keepdims=True))).astype(jnp.float32)
        partial_value = jnp.einsum('thd,ehd->the', query_grad, query_heads) + gate_grad[..., None] * gate_float[None]
        token_rows = lax.optimization_barrier(jnp.sum(to_low(partial_value).astype(jnp.float32), axis=1)).astype(jnp.bfloat16)
        return (token_rows, khat_grad, value_grad)
    token_rows, khat_all, value_all = lax.map(reader, jnp.arange(N_ST, dtype=jnp.int32))
    owner_all, local_all, rank_all = request_slots(every_id, PASS_DEV)
    cap_iota = jnp.arange(CAP, dtype=jnp.int32)
    req_iota = jnp.arange(REQ_DEV, dtype=jnp.int32)
    readers = jnp.arange(N_ST, dtype=jnp.int32)[:, None]
    pass_iota = jnp.arange(PASS_DEV, dtype=jnp.int32)

    def owner_step(weight_acc, owner_idx):
        wanted = (owner_all == owner_idx)[:, None, :] & (rank_all[:, None, :] == cap_iota[None, :, None])
        slot_used = jnp.any(wanted, axis=-1)
        slot_local = lax.optimization_barrier(jnp.sum(jnp.where(wanted, local_all[:, None, :], 0), axis=-1, dtype=jnp.int32))
        req_pick = lax.optimization_barrier(jnp.sum(jnp.where(wanted, req_iota[None, None, :], 0), axis=-1, dtype=jnp.int32))
        khat_slots = jnp.where(slot_used[:, :, None, None, None], khat_all[readers, req_pick], 0.0)
        value_slots = jnp.where(slot_used[:, :, None, None, None], value_all[readers, req_pick], 0.0)
        onehot = ((slot_local.reshape(-1)[None, :] == pass_iota[:, None]) & slot_used.reshape(-1)[None, :]).astype(jnp.float32)
        khat_pass = jnp.dot(onehot, khat_slots.reshape(N_ST * CAP, -1), precision=HIGHEST).reshape(PASS_DEV * PROWS, HEADS, HEAD)
        value_pass = jnp.dot(onehot, value_slots.reshape(N_ST * CAP, -1), precision=HIGHEST).reshape(PASS_DEV * PROWS, HEADS, HEAD)
        row_block = lax.dynamic_slice_in_dim(passages, owner_idx * PASS_DEV, PASS_DEV, 0).reshape(PASS_DEV * PROWS, D)
        key_low = to_low(jnp.dot(row_block, key_weight, preferred_element_type=jnp.float32))
        key_float = key_low.astype(jnp.float32).reshape(PASS_DEV * PROWS, HEADS, HEAD)
        key_scale = lax.rsqrt(lax.optimization_barrier(jnp.mean(key_float * key_float, axis=-1, keepdims=True)) + NORM_FLOOR)
        key_grad = to_low(key_scale * khat_pass - key_scale ** 3 * key_float * lax.optimization_barrier(jnp.mean(key_float * khat_pass, axis=-1, keepdims=True)))
        value_grad_low = to_low(value_pass)
        partial_value = jnp.einsum('rhd,ehd->rhe', key_grad.astype(jnp.float32), key_heads) + jnp.einsum('rhd,ehd->rhe', value_grad_low.astype(jnp.float32), value_heads)
        rows_grad = lax.optimization_barrier(jnp.sum(to_low(partial_value).astype(jnp.float32), axis=1)).astype(jnp.bfloat16).reshape(PASS_DEV, PROWS, D)
        weight_acc = weight_acc + jnp.dot(row_block.T, key_grad.reshape(PASS_DEV * PROWS, HEADS * HEAD), preferred_element_type=jnp.float32)
        return (weight_acc, rows_grad)
    weight_grad, store_grad = lax.scan(owner_step, jnp.zeros((D, HEADS * HEAD), jnp.float32), jnp.arange(N_ST, dtype=jnp.int32))
    return (token_rows.reshape(TOKENS, D), store_grad.reshape(PASSAGES, PROWS, D), weight_grad)
```

```python
import functools

import jax
import jax.numpy as jnp
from jax import lax
from jax.experimental import pallas as pl
from jax.experimental.pallas import tpu as pltpu
from jax.sharding import Mesh
from jax.sharding import PartitionSpec as P

SPAN = 64
ST = ("z", "y", "c")
NORM_FLOOR = 1.0
SCORE_GAIN = 4.0
CONTRACT_LAST = (((1,), (1,)), ((), ()))
CONTRACT_FIRST = (((0,), (0,)), ((), ()))
BF = jnp.bfloat16
F32 = jnp.float32


def shift(value, axis, step):
    n = lax.axis_size(axis)
    return lax.ppermute(value, axis, [(i, (i + step) % n) for i in range(n)])


def low_dot(a, b, dims=(((1,), (0,)), ((), ()))):
    return lax.dot_general(a.astype(BF), b.astype(BF), dims, preferred_element_type=F32)


def mixer_kernel(q_ref, k_ref, v_ref, cot_ref, rows_ref, cols_ref, out_ref):
    length, width = q_ref.shape
    heads_n = 2
    dim = width // heads_n
    blocks_n = length // SPAN
    at = lax.broadcasted_iota(jnp.int32, (SPAN, SPAN), 0)
    to = lax.broadcasted_iota(jnp.int32, (SPAN, SPAN), 1)
    eye = (at == to).astype(F32)
    pairs = [(h, n) for n in range(blocks_n) for h in range(heads_n)]
    held = {}
    for h, n in pairs:
        part = (slice(n * SPAN, (n + 1) * SPAN), slice(h * dim, (h + 1) * dim))
        q, k, v = (ref[part].astype(F32) for ref in (q_ref, k_ref, v_ref))
        q = q * lax.rsqrt(jnp.sum(q * q, axis=1, keepdims=True) + NORM_FLOOR) * dim ** (-0.5)
        k = k * lax.rsqrt(jnp.sum(k * k, axis=1, keepdims=True) + NORM_FLOOR)
        m = h * blocks_n + n
        cum_row = rows_ref[m : m + 1, :]
        cum = cols_ref[:, m : m + 1]
        strength = cols_ref[:, 2 * blocks_n + m : 2 * blocks_n + m + 1]
        last = rows_ref[m : m + 1, SPAN - 1 : SPAN]
        decay = jnp.exp(jnp.where(at >= to, cum - cum_row, -jnp.inf))
        grow = jnp.exp(cum)
        strict = jnp.where(at > to, strength * low_dot(k, k, CONTRACT_LAST) * decay, 0.0)
        attend = jnp.where(at >= to, low_dot(q, k, CONTRACT_LAST) * decay, 0.0).astype(BF)
        right = jnp.concatenate([v * strength, k * (strength * grow)], axis=1).astype(BF)
        held[h, n] = [
            strict,
            right,
            attend,
            (q * grow).astype(BF),
            (k * jnp.exp(last - cum)).astype(BF),
            jnp.exp(last),
        ]
    running = {p: eye - held[p][0] for p in pairs}
    power = {p: held[p][0] for p in pairs}
    for _ in range(SPAN.bit_length() - 2):
        for p in pairs:
            power[p] = low_dot(power[p], power[p])
        for p in pairs:
            running[p] = low_dot(running[p], eye + power[p])
    solved = {p: low_dot(running[p], held[p][1]) for p in pairs}
    state = [jnp.zeros((dim, dim), F32) for _ in range(heads_n)]
    for n in range(blocks_n):
        rows = slice(n * SPAN, (n + 1) * SPAN)
        total = 0.0
        for h in range(heads_n):
            _, _, attend, q_dec, k_dec, carry = held[h, n]
            s_low = state[h].astype(BF)
            fresh = (solved[h, n][:, :dim] - low_dot(solved[h, n][:, dim:], s_low)).astype(BF)
            out = low_dot(q_dec, s_low) + low_dot(attend, fresh)
            state[h] = state[h] * carry + low_dot(k_dec, fresh, CONTRACT_FIRST)
            cot = cot_ref[rows, h * dim : (h + 1) * dim].astype(F32)
            total = total + jnp.sum(out * cot, axis=1, keepdims=True)
        out_ref[rows, :] = total


def mixer_dot(query_raw, key_raw, value_raw, cotangent, beta_raw, decay_raw, rate_vals):
    strength = jax.nn.sigmoid(beta_raw).reshape(-1, SPAN)
    log_decay = (-rate_vals[:, None] * jax.nn.softplus(decay_raw)).reshape(-1, SPAN)
    upto = (jnp.arange(SPAN)[:, None] <= jnp.arange(SPAN)[None, :]).astype(F32)
    cumulative = jnp.dot(log_decay, upto, precision=lax.Precision.HIGHEST)
    columns = jnp.concatenate([cumulative, strength], axis=0).T
    vmem = pl.BlockSpec(memory_space=pltpu.VMEM)
    return pl.pallas_call(
        mixer_kernel,
        out_shape=jax.ShapeDtypeStruct((query_raw.shape[0], 1), F32),
        in_specs=[vmem] * 6,
        out_specs=vmem,
        name="mixer",
    )(query_raw, key_raw, value_raw, cotangent, cumulative, columns)


def fetch(pos_ref, q_refs, c_refs, kv_refs, qs, cs, kvs, sems):
    z = pos_ref[0]
    rows = q_refs[0].shape[0]
    half_blocks = q_refs[8].shape[0]
    copies = []

    def add(src, dst):
        copies.append(pltpu.make_async_copy(src, dst, sems.at[len(copies)]))

    for pieces, store in ((q_refs, qs), (c_refs, cs)):
        for rel in range(8):
            slot = (z + rel) & 7
            if rel == 4:
                add(pieces[4], store.at[slot, pl.ds(0, half_blocks)])
                add(pieces[8], store.at[slot, pl.ds(half_blocks, half_blocks)])
            else:
                add(pieces[rel], store.at[slot])
    for other in range(2):
        own, plus, far_a, far_b, minus = kv_refs[5 * other : 5 * other + 5]
        per = own.shape[0]
        for rel, ref in ((0, own), (1, plus), (3, minus)):
            add(ref, kvs.at[pl.ds((rel * 2 + other) * per, per)])
        base = (4 + other) * per
        add(far_a, kvs.at[pl.ds(base, per // 2)])
        add(far_b, kvs.at[pl.ds(base + per // 2, per // 2)])
    for copy in copies:
        copy.start()
    return copies


def split_code(code):
    row = code >> 7
    return row, row // 6, row % 6, code & 127


def pair_scores(scale, q, cot, kv):
    head = q.shape[-1]
    scores = lax.dot_general(kv[:, :head], q, CONTRACT_LAST, preferred_element_type=F32) * scale
    grads = lax.dot_general(kv[:, head:], cot, CONTRACT_LAST, preferred_element_type=F32)
    return jnp.exp(scores), grads


def sums_kernel(scale, ids_ref, pos_ref, *refs):
    q_refs, c_refs, kv_refs = refs[:9], refs[9:18], refs[18:28]
    out_ref, code_ref, count_ref, qs, cs, kvs, sems = refs[28:]
    copies = fetch(pos_ref, q_refs, c_refs, kv_refs, qs, cs, kvs, sems)
    out_ref[...] = jnp.zeros_like(out_ref)
    z, y, c = pos_ref[0], pos_ref[1], pos_ref[2]
    per_owner = kvs.shape[0] // 8
    per_block = ids_ref.shape[0] // out_ref.shape[0]

    def clear(i, carry):
        code_ref[i] = 0
        return carry

    lax.fori_loop(0, code_ref.shape[0], clear, 0)

    def collect(row, found):
        for j in range(per_block):
            one = ids_ref[row * per_block + j]
            lane = (one // per_owner) & 7
            slot = ((((lane >> 1) - y) & 3) * 2 + ((lane & 1) ^ c)) * per_owner + one % per_owner
            code_ref[found] = row * 128 + slot
            found = found + (one // (8 * per_owner) == z).astype(jnp.int32)
        return found

    count = lax.fori_loop(0, out_ref.shape[0], collect, jnp.int32(0))
    code_ref[count] = 0
    count_ref[0] = count
    for copy in copies:
        copy.wait()

    def step(i, carry):
        done = []
        for u in range(2):
            at = 2 * i + u
            row, reader, block, slot = split_code(code_ref[at])
            e, g = pair_scores(scale, qs[reader, block], cs[reader, block], kvs[slot])
            both = jnp.concatenate(
                [jnp.sum(e, axis=0, keepdims=True), jnp.sum(e * g, axis=0, keepdims=True)], axis=1
            )
            done.append((row, jnp.where(at < count, both, 0.0)))
        for row, both in done:
            out_ref[pl.ds(row, 1), :] += both
        return carry

    lax.fori_loop(0, (count + 1) // 2, step, 0)


def terms_kernel(scale, code_ref, count_ref, pos_ref, tot_ref, gate_ref, *refs):
    q_refs, c_refs, kv_refs = refs[:9], refs[9:18], refs[18:28]
    part_refs, qout_ref = refs[28:44], refs[44]
    qs, cs, kvs, acc, qacc, sems = refs[45:]
    copies = fetch(pos_ref, q_refs, c_refs, kv_refs, qs, cs, kvs, sems)
    acc[...] = jnp.zeros_like(acc)
    qacc[...] = jnp.zeros_like(qacc)
    for copy in copies:
        copy.wait()
    count = count_ref[0]
    span = gate_ref.shape[-1]

    def step(i, carry):
        done = []
        for u in range(2):
            at = 2 * i + u
            row, reader, block, slot = split_code(code_ref[at])
            q, cot, kv = qs[reader, block], cs[reader, block], kvs[slot]
            e, g = pair_scores(scale, q, cot, kv)
            tot = tot_ref[pl.ds(row, 1), :]
            gated = e * (gate_ref[pl.ds(row, 1), :] / tot[:, :span])
            low = gated.astype(BF)
            grad = (gated * (g - tot[:, span:])).astype(BF)
            key_term = lax.dot_general(
                grad, q, (((1,), (0,)), ((), ())), preferred_element_type=F32
            ) * scale
            value_term = lax.dot_general(
                low, cot, (((1,), (0,)), ((), ())), preferred_element_type=F32
            )
            q_term = lax.dot_general(
                grad, kv[:, : q.shape[-1]], CONTRACT_FIRST, preferred_element_type=F32
            ) * scale
            both = jnp.concatenate([key_term, value_term], axis=1).astype(BF).astype(F32)
            valid = at < count
            done.append((slot, reader, block, jnp.where(valid, both, 0.0), jnp.where(valid, q_term, 0.0)))
        for slot, reader, block, both, q_term in done:
            acc[slot] = (acc[slot].astype(F32) + both).astype(BF)
            qacc[reader, block] += q_term
        return carry

    lax.fori_loop(0, (count + 1) // 2, step, 0)
    outs = []
    half = part_refs[0].shape[0]
    for n, ref in enumerate(part_refs):
        copy = pltpu.make_async_copy(acc.at[pl.ds(n * half, half)], ref, sems.at[n])
        copy.start()
        outs.append(copy)
    qout_ref[...] = qacc[...].astype(BF)
    for copy in outs:
        copy.wait()


def ring4(value, axis):
    half = value.shape[0] // 2
    below = shift(value, axis, 1)
    above = shift(value, axis, -1)
    far_a = shift(below[:half], axis, 1)
    far_b = shift(above[half:], axis, -1)
    return value, above, far_a, far_b, below


def ring8(value, axis):
    half = value.shape[0] // 2
    below, above = [value], [value]
    for _ in range(3):
        below.append(shift(below[-1], axis, 1))
        above.append(shift(above[-1], axis, -1))
    far_a = shift(below[3][:half], axis, 1)
    far_b = shift(above[3][half:], axis, -1)
    return [value, above[1], above[2], above[3], far_a, below[3], below[2], below[1], far_b]


def swap(value):
    return lax.ppermute(value, "c", [(0, 1), (1, 0)])


def copy_for_each(shard, axis):
    copies = jnp.broadcast_to(shard, (lax.axis_size(axis), *shard.shape))
    return lax.all_to_all(copies, axis, split_axis=0, concat_axis=0, tiled=True)


def body(
    tokens,
    cotangent,
    mix_query,
    mix_key,
    mix_value,
    beta_pre,
    decay_pre,
    decay_rate,
    passages,
    passage_ids,
    query_weight,
    key_weight,
    value_weight,
    gate_weight,
):
    tok_rows = tokens.shape[0]
    width, head = query_weight.shape
    per_owner, rows_each = passages.shape[:2]
    blocks_n, per_block = passage_ids.shape
    span = tok_rows // blocks_n
    scale = SCORE_GAIN * head ** (-0.5)
    z, y, c, x = (lax.axis_index(a) for a in ("z", "y", "c", "x"))
    slice_w = width // 4

    ids = copy_for_each(passage_ids, "z").reshape(-1)
    pos = jnp.stack([z, y, c]).astype(jnp.int32)

    flat_rows = passages.reshape(per_owner * rows_each, width)
    key_low = lax.optimization_barrier(
        jnp.dot(flat_rows, key_weight, preferred_element_type=F32).astype(BF)
    )
    value_all = jnp.dot(flat_rows, value_weight, preferred_element_type=F32).astype(BF)
    key_float = key_low.astype(F32)
    key_scale = lax.rsqrt(jnp.mean(key_float * key_float, axis=-1, keepdims=True) + NORM_FLOOR)
    key_hat = (key_float * key_scale).astype(BF)
    packed = jnp.concatenate([key_hat, value_all], axis=-1).reshape(per_owner, rows_each, 2 * head)
    kv_pieces = ring4(packed, "y")
    kv_pieces = tuple(kv_pieces) + tuple(swap(piece) for piece in kv_pieces)

    wq_turned = lax.dynamic_slice_in_dim(
        jnp.concatenate([query_weight, query_weight], axis=0), x * slice_w, width, 0
    )
    gw_turned = lax.dynamic_slice_in_dim(
        jnp.concatenate([gate_weight, gate_weight], axis=1), x * slice_w, width, 1
    )
    tok_own, tok_up, tok_far_a, tok_far_b, tok_down = ring4(tokens, "x")
    tok_far = jnp.concatenate([tok_far_a, tok_far_b], axis=0)
    query_acc = 0.0
    gate_acc = 0.0
    for n, piece in enumerate((tok_own, tok_up, tok_far, tok_down)):
        query_acc = query_acc + jnp.dot(
            piece, wq_turned[n * slice_w : (n + 1) * slice_w], preferred_element_type=F32
        )
        gate_acc = gate_acc + jnp.sum(
            piece.astype(F32) * gw_turned[:, n * slice_w : (n + 1) * slice_w].astype(F32), axis=1
        )
    query_low = lax.optimization_barrier(query_acc.astype(BF))
    query_float = query_low.astype(F32)
    query_scale = lax.rsqrt(
        jnp.mean(query_float * query_float, axis=-1, keepdims=True) + NORM_FLOOR
    )
    query_hat = (query_float * query_scale).astype(BF)
    gate_open = jax.nn.sigmoid(gate_acc)
    c_pieces = ring8(cotangent.reshape(blocks_n, span, head), "z")
    q_pieces = ring8(query_hat.reshape(blocks_n, span, head), "z")

    any_space = pl.BlockSpec(memory_space=pl.ANY)
    smem = pl.BlockSpec(memory_space=pltpu.SMEM)
    vmem = pl.BlockSpec(memory_space=pltpu.VMEM)
    stores = [
        pltpu.VMEM((8, blocks_n, span, head), BF),
        pltpu.VMEM((8, blocks_n, span, head), BF),
        pltpu.VMEM((8 * per_owner, rows_each, 2 * head), BF),
    ]
    pieces = (*q_pieces, *c_pieces, *kv_pieces)
    params = pltpu.CompilerParams(vmem_limit_bytes=60 * 1024 * 1024)
    partial, codes, count = pl.pallas_call(
        functools.partial(sums_kernel, scale),
        out_shape=[
            jax.ShapeDtypeStruct((8 * blocks_n, 2 * span), F32),
            jax.ShapeDtypeStruct((72,), jnp.int32),
            jax.ShapeDtypeStruct((1,), jnp.int32),
        ],
        in_specs=[smem, smem] + [any_space] * 28,
        out_specs=[vmem, smem, smem],
        scratch_shapes=stores + [pltpu.SemaphoreType.DMA((28,))],
        compiler_params=params,
        name="sums",
    )(ids, pos, *pieces)

    gate_column = jnp.pad(
        jnp.broadcast_to(gate_weight.reshape(width, 1), (width, 2)), ((0, 0), (0, 126))
    )
    weights = jnp.concatenate([key_weight, value_weight, query_weight, gate_column], axis=1)
    weights, _ = lax.optimization_barrier((weights, partial))
    weights = weights.reshape(4, slice_w, weights.shape[1])

    def weight_rows(step):
        rows = lax.dynamic_index_in_dim(weights, (x + step) & 3, 0, keepdims=False)
        return rows if step == 0 else shift(rows, "x", step)

    w_own, w_down, w_up, w_far = (weight_rows(s) for s in (0, 1, -1, 2))

    gate_rows = jnp.pad(gate_open.reshape(blocks_n, span), ((0, 0), (0, span)))
    arrived = copy_for_each(jnp.concatenate([partial, gate_rows], axis=0)[None], "z").reshape(
        8, 9 * blocks_n, 2 * span
    )
    summed = jnp.sum(arrived[:, : 8 * blocks_n], axis=0)
    totals = jnp.concatenate([summed[:, :span], summed[:, span:] / summed[:, :span]], axis=1)
    gates = arrived[:, 8 * blocks_n :, :span].reshape(8 * blocks_n, span)

    half_shape = (per_owner // 2, rows_each, 2 * head)
    results = pl.pallas_call(
        functools.partial(terms_kernel, scale),
        out_shape=[jax.ShapeDtypeStruct(half_shape, BF)] * 16
        + [jax.ShapeDtypeStruct((8, blocks_n, span, head), BF)],
        in_specs=[smem, smem, smem, vmem, vmem] + [any_space] * 28,
        out_specs=[any_space] * 16 + [vmem],
        scratch_shapes=stores
        + [
            pltpu.VMEM((8 * per_owner, rows_each, 2 * head), BF),
            pltpu.VMEM((8, blocks_n, span, head), F32),
            pltpu.SemaphoreType.DMA((28,)),
        ],
        compiler_params=params,
        name="terms",
    )(codes, count, pos, totals, gates, *pieces)

    def plus(a, b):
        return (a.astype(F32) + b.astype(F32)).astype(BF)

    def block(rel, half):
        return plus(results[rel * 4 + half], swap(results[rel * 4 + 2 + half]))

    far_a, far_b = block(2, 0), block(2, 1)
    near_a, near_b = block(1, 0), block(1, 1)
    back_a, back_b = block(3, 0), block(3, 1)
    got_a = shift(far_a, "y", 1)
    got_b = shift(far_b, "y", -1)
    early_b = shift(near_b, "y", 1)
    early_a = shift(back_a, "y", -1)
    late_a = shift(plus(near_a, got_a), "y", 1)
    late_b = shift(plus(back_b, got_b), "y", -1)
    sums = []
    for half, one, two in ((0, early_a, late_a), (1, early_b, late_b)):
        sums.append(
            results[half].astype(F32)
            + swap(results[2 + half]).astype(F32)
            + one.astype(F32)
            + two.astype(F32)
        )

    q_back = lax.all_to_all(results[16], "z", split_axis=0, concat_axis=0, tiled=True)
    qhat_grad = jnp.sum(q_back.astype(F32), axis=0).reshape(tok_rows, head)
    query_grad = (
        query_scale * qhat_grad
        - query_scale**3 * query_float * jnp.mean(query_float * qhat_grad, axis=-1, keepdims=True)
    ).astype(BF)
    mix_query, _ = lax.optimization_barrier((mix_query, results[16]))
    mixed_dot = mixer_dot(
        mix_query, mix_key, mix_value, cotangent, beta_pre, decay_pre, decay_rate
    ).reshape(tok_rows)
    own_totals = lax.dynamic_slice_in_dim(totals, z * blocks_n, blocks_n, 0)
    retrieved_dot = own_totals[:, span:].reshape(tok_rows)
    gate_grad = (retrieved_dot - mixed_dot) * gate_open * (1.0 - gate_open)
    high = gate_grad.astype(BF)
    rest = (gate_grad - high.astype(F32)).astype(BF)
    columns = jnp.pad(jnp.stack([high, rest], axis=1), ((0, 0), (0, 126)))
    token_send = jnp.concatenate([query_grad, columns], axis=1)
    g_own, g_up, g_far_a, g_far_b, g_down = ring4(token_send, "x")
    g_far = jnp.concatenate([g_far_a, g_far_b], axis=0)
    token_sum = 0.0
    for piece, rows in ((g_own, w_own), (g_up, w_up), (g_down, w_down), (g_far, w_far)):
        term = lax.dot_general(piece, rows[:, 2 * head :], CONTRACT_LAST, preferred_element_type=F32)
        token_sum = token_sum + term.astype(BF).astype(F32)
    token_grad = token_sum.astype(BF)

    row_grads = []
    weight_term = 0.0
    half_rows = per_owner * rows_each // 2
    for half in range(2):
        part = slice(half * half_rows, (half + 1) * half_rows)
        total = sums[half].reshape(half_rows, 2 * head)
        kf, ks = key_float[part], key_scale[part]
        hat_grad = total[:, :head]
        key_grad = (
            ks * hat_grad - ks**3 * kf * jnp.mean(kf * hat_grad, axis=-1, keepdims=True)
        ).astype(BF)
        row_grads.append(jnp.concatenate([key_grad, total[:, head:].astype(BF)], axis=1))
    key_grad = jnp.concatenate([g[:, :head] for g in row_grads], axis=0)
    weight_term = lax.dot_general(flat_rows, key_grad, CONTRACT_FIRST, preferred_element_type=F32)
    weight_back = lax.all_to_all(
        weight_term.astype(BF).reshape(64, width // 64, head), ST, split_axis=0, concat_axis=0, tiled=True
    )
    key_weight_grad = jnp.sum(weight_back.astype(F32), axis=0)
    up = [shift(g, "x", -1) for g in row_grads]
    down = [shift(g, "x", 1) for g in row_grads]
    far = [shift(down[0], "x", 1), shift(up[1], "x", -1)]
    grads = []
    for half in range(2):
        row_sum = 0.0
        for piece, rows in (
            (row_grads[half], w_own),
            (up[half], w_up),
            (down[half], w_down),
            (far[half], w_far),
        ):
            term = lax.dot_general(
                piece, rows[:, : 2 * head], CONTRACT_LAST, preferred_element_type=F32
            )
            row_sum = row_sum + term.astype(BF).astype(F32)
        grads.append(row_sum.astype(BF))
    passage_grad = jnp.concatenate(grads, axis=0).reshape(per_owner, rows_each, slice_w)
    return (token_grad, passage_grad, key_weight_grad)


def solution(mesh):
    torus = Mesh(mesh.devices.reshape(8, 4, 2, mesh.shape["tp"]), ("z", "y", "c", "x"))
    return jax.shard_map(
        body,
        mesh=torus,
        in_specs=(
            P(ST, "x"),
            P(ST, "x"),
            P(ST, "x"),
            P(ST, "x"),
            P(ST, "x"),
            P("x", ST),
            P("x", ST),
            P("x"),
            P(ST, None, None),
            P(ST, None),
            P(None, "x"),
            P(None, "x"),
            P(None, "x"),
            P("x", None),
        ),
        out_specs=(P(ST, "x"), P(ST, None, "x"), P(ST, "x")),
        check_vma=False,
    )
```

```python
import functools

import jax
import jax.numpy as jnp
from jax import lax
from jax.experimental import pallas as pl
from jax.experimental.pallas import tpu as pltpu
from jax.sharding import Mesh
from jax.sharding import PartitionSpec as P


SPAN = 64
ST = ("z", "y", "c")
NORM_FLOOR = 1.0
SCORE_GAIN = 4.0
CONTRACT_LAST = (((1,), (1,)), ((), ()))
CONTRACT_FIRST = (((0,), (0,)), ((), ()))
BF = jnp.bfloat16
F32 = jnp.float32


def shift(value, axis, step):
    n = lax.axis_size(axis)
    return lax.ppermute(value, axis, [(i, (i + step) % n) for i in range(n)])


def low_dot(a, b, dims=(((1,), (0,)), ((), ()))):
    return lax.dot_general(a.astype(BF), b.astype(BF), dims, preferred_element_type=F32)


def mixer_kernel(q_ref, k_ref, v_ref, cot_ref, rows_ref, cols_ref, out_ref):
    length, width = q_ref.shape
    heads_n = 2
    dim = width // heads_n
    blocks_n = length // SPAN
    at = lax.broadcasted_iota(jnp.int32, (SPAN, SPAN), 0)
    to = lax.broadcasted_iota(jnp.int32, (SPAN, SPAN), 1)
    eye = (at == to).astype(F32)
    pairs = [(h, n) for n in range(blocks_n) for h in range(heads_n)]
    held = {}
    for h, n in pairs:
        part = (slice(n * SPAN, (n + 1) * SPAN), slice(h * dim, (h + 1) * dim))
        q, k, v = (ref[part].astype(F32) for ref in (q_ref, k_ref, v_ref))
        q = q * lax.rsqrt(jnp.sum(q * q, axis=1, keepdims=True) + NORM_FLOOR) * dim ** (-0.5)
        k = k * lax.rsqrt(jnp.sum(k * k, axis=1, keepdims=True) + NORM_FLOOR)
        m = h * blocks_n + n
        cum_row = rows_ref[m : m + 1, :]
        cum = cols_ref[:, m : m + 1]
        strength = cols_ref[:, 2 * blocks_n + m : 2 * blocks_n + m + 1]
        last = rows_ref[m : m + 1, SPAN - 1 : SPAN]
        decay = jnp.exp(jnp.where(at >= to, cum - cum_row, -jnp.inf))
        grow = jnp.exp(cum)
        strict = jnp.where(at > to, strength * low_dot(k, k, CONTRACT_LAST) * decay, 0.0)
        attend = jnp.where(at >= to, low_dot(q, k, CONTRACT_LAST) * decay, 0.0).astype(BF)
        right = jnp.concatenate([v * strength, k * (strength * grow)], axis=1).astype(BF)
        held[h, n] = [
            strict,
            right,
            attend,
            (q * grow).astype(BF),
            (k * jnp.exp(last - cum)).astype(BF),
            jnp.exp(last),
        ]
    running = {p: eye - held[p][0] for p in pairs}
    power = {p: held[p][0] for p in pairs}
    for _ in range(SPAN.bit_length() - 2):
        for p in pairs:
            power[p] = low_dot(power[p], power[p])
        for p in pairs:
            running[p] = low_dot(running[p], eye + power[p])
    solved = {p: low_dot(running[p], held[p][1]) for p in pairs}
    state = [jnp.zeros((dim, dim), F32) for _ in range(heads_n)]
    for n in range(blocks_n):
        rows = slice(n * SPAN, (n + 1) * SPAN)
        total = 0.0
        for h in range(heads_n):
            _, _, attend, q_dec, k_dec, carry = held[h, n]
            s_low = state[h].astype(BF)
            fresh = (solved[h, n][:, :dim] - low_dot(solved[h, n][:, dim:], s_low)).astype(BF)
            out = low_dot(q_dec, s_low) + low_dot(attend, fresh)
            state[h] = state[h] * carry + low_dot(k_dec, fresh, CONTRACT_FIRST)
            cot = cot_ref[rows, h * dim : (h + 1) * dim].astype(F32)
            total = total + jnp.sum(out * cot, axis=1, keepdims=True)
        out_ref[rows, :] = total


def mixer_dot(query_raw, key_raw, value_raw, cotangent, beta_raw, decay_raw, rate_vals):
    strength = jax.nn.sigmoid(beta_raw).reshape(-1, SPAN)
    log_decay = (-rate_vals[:, None] * jax.nn.softplus(decay_raw)).reshape(-1, SPAN)
    upto = (jnp.arange(SPAN)[:, None] <= jnp.arange(SPAN)[None, :]).astype(F32)
    cumulative = jnp.dot(log_decay, upto, precision=lax.Precision.HIGHEST)
    columns = jnp.concatenate([cumulative, strength], axis=0).T
    vmem = pl.BlockSpec(memory_space=pltpu.VMEM)
    return pl.pallas_call(
        mixer_kernel,
        out_shape=jax.ShapeDtypeStruct((query_raw.shape[0], 1), F32),
        in_specs=[vmem] * 6,
        out_specs=vmem,
        name="mixer",
    )(query_raw, key_raw, value_raw, cotangent, cumulative, columns)


def fetch(pos_ref, q_refs, c_ref, kv_refs, qs, cs, kvs, sems):
    z = pos_ref[0]
    rows = qs.shape[1]
    copies = []

    def add(src, dst):
        copies.append(pltpu.make_async_copy(src, dst, sems.at[len(copies)]))

    for rel in range(8):
        slot = (z + rel) & 7
        if rel == 4:
            add(q_refs[4], qs.at[slot, pl.ds(0, rows // 2)])
            add(q_refs[8], qs.at[slot, pl.ds(rows // 2, rows // 2)])
        else:
            add(q_refs[rel], qs.at[slot])
    add(c_ref.at[:, pl.ds(0, rows)], cs)
    for other in range(2):
        own, plus, far_a, far_b, minus = kv_refs[5 * other : 5 * other + 5]
        per = own.shape[0]
        for rel, ref in ((0, own), (1, plus), (3, minus)):
            add(ref, kvs.at[pl.ds((other * 4 + ((rel + 2) & 3)) * per, per)])
        base = other * 4 * per
        add(far_a, kvs.at[pl.ds(base, per // 2)])
        add(far_b, kvs.at[pl.ds(base + per // 2, per // 2)])
    for copy in copies:
        copy.start()
    return copies


def split_code(code):
    row = code >> 7
    return row, row // 6, row % 6, code & 127


def pair_scores(scale, q, cot, kv):
    head = q.shape[-1]
    scores = lax.dot_general(kv[:, :head], q, CONTRACT_LAST, preferred_element_type=F32) * scale
    grads = lax.dot_general(kv[:, head:], cot, CONTRACT_LAST, preferred_element_type=F32)
    return jnp.exp(scores), grads


def sums_kernel(scale, ids_ref, pos_ref, gate_ref, *refs):
    q_refs, c_ref, kv_refs = refs[:9], refs[9], refs[10:20]
    out_ref, code_ref, count_ref, qs, cs, kvs, sems = refs[20:]
    copies = fetch(pos_ref, q_refs, c_ref, kv_refs, qs, cs, kvs, sems)
    blocks_n, span = gate_ref.shape
    blocks_all = 8 * blocks_n
    out_ref[...] = jnp.zeros_like(out_ref)
    z, y, c = pos_ref[0], pos_ref[1], pos_ref[2]
    per_owner = kvs.shape[0] // 8
    per_block = ids_ref.shape[0] // blocks_all

    def clear(i, carry):
        code_ref[i] = 0
        return carry

    lax.fori_loop(0, code_ref.shape[0], clear, 0)

    def collect(row, found):
        for j in range(per_block):
            one = ids_ref[row * per_block + j]
            lane = (one // per_owner) & 7
            place = ((lane & 1) ^ c) * 4 + (((lane >> 1) - y + 2) & 3)
            code_ref[found] = row * 128 + place * per_owner + one % per_owner
            found = found + (one // (8 * per_owner) == z).astype(jnp.int32)
        return found

    count = lax.fori_loop(0, blocks_all, collect, jnp.int32(0))
    code_ref[count] = 0
    count_ref[0] = count
    for copy in copies:
        copy.wait()

    def step(i, carry):
        done = []
        for u in range(2):
            at = 2 * i + u
            row, reader, block, slot = split_code(code_ref[at])
            tok = pl.ds(pl.multiple_of(block * span, span), span)
            e, g = pair_scores(scale, qs[reader, tok], cs[reader, tok], kvs[slot])
            both = jnp.concatenate(
                [jnp.sum(e, axis=0, keepdims=True), jnp.sum(e * g, axis=0, keepdims=True)], axis=1
            )
            done.append((row, jnp.where(at < count, both, 0.0)))
        for row, both in done:
            out_ref[0, pl.ds(row, 1), :] += both
        return carry

    lax.fori_loop(0, (count + 1) // 2, step, 0)
    out_ref[0, blocks_all : blocks_all + blocks_n, 0:span] = gate_ref[...]
    for i in range(1, 8):
        out_ref[i] = out_ref[0]


def terms_kernel(scale, code_ref, count_ref, pos_ref, arrived_ref, *refs):
    q_refs, c_ref, kv_refs = refs[:9], refs[9], refs[10:20]
    part_refs, qout_ref, tot_ref = refs[20:24], refs[24], refs[25]
    qs, cs, kvs, acc, qacc, gates, sems = refs[26:]
    copies = fetch(pos_ref, q_refs, c_ref, kv_refs, qs, cs, kvs, sems)
    acc[...] = jnp.zeros_like(acc)
    qacc[...] = jnp.zeros_like(qacc)
    count = count_ref[0]
    blocks_all = tot_ref.shape[0]
    span = tot_ref.shape[1] // 2
    blocks_n = blocks_all // 8
    summed = jnp.sum(arrived_ref[:, :blocks_all, :], axis=0)
    lanes = lax.broadcasted_iota(jnp.int32, summed.shape, 1)
    weights = jnp.concatenate([summed[:, :span], summed[:, :span]], axis=1)
    tot_ref[...] = jnp.where(lanes < span, summed, summed / weights)
    for i in range(8):
        gates[i * blocks_n : (i + 1) * blocks_n, :] = arrived_ref[
            i, blocks_all : blocks_all + blocks_n, :
        ]
    for copy in copies:
        copy.wait()

    def step(i, carry):
        done = []
        for u in range(2):
            at = 2 * i + u
            row, reader, block, slot = split_code(code_ref[at])
            tok = pl.ds(pl.multiple_of(block * span, span), span)
            q, cot, kv = qs[reader, tok], cs[reader, tok], kvs[slot]
            e, g = pair_scores(scale, q, cot, kv)
            tot = tot_ref[pl.ds(row, 1), :]
            gated = e * (gates[pl.ds(row, 1), :][:, :span] / tot[:, :span])
            low = gated.astype(BF)
            grad = (gated * (g - tot[:, span:])).astype(BF)
            key_term = lax.dot_general(
                grad, q, (((1,), (0,)), ((), ())), preferred_element_type=F32
            ) * scale
            value_term = lax.dot_general(
                low, cot, (((1,), (0,)), ((), ())), preferred_element_type=F32
            )
            q_term = lax.dot_general(
                grad, kv[:, : q.shape[-1]], CONTRACT_FIRST, preferred_element_type=F32
            ) * scale
            both = jnp.concatenate([key_term, value_term], axis=1).astype(BF).astype(F32)
            valid = at < count
            done.append((slot, reader, tok, jnp.where(valid, both, 0.0), jnp.where(valid, q_term, 0.0)))
        for slot, reader, tok, both, q_term in done:
            acc[slot] = (acc[slot].astype(F32) + both).astype(BF)
            qacc[reader, tok] += q_term
        return carry

    lax.fori_loop(0, (count + 1) // 2, step, 0)
    outs = []
    order = (2, 0, 3, 1)
    starts = {0: 0, 1: part_refs[0].shape[0]}
    starts[2] = starts[1] + part_refs[1].shape[0]
    starts[3] = starts[2] + part_refs[2].shape[0]
    for n in order:
        ref = part_refs[n]
        copy = pltpu.make_async_copy(acc.at[pl.ds(starts[n], ref.shape[0])], ref, sems.at[n])
        copy.start()
        outs.append(copy)
    qout_ref[...] = qacc[...].astype(BF)
    for copy in outs:
        copy.wait()


def finish_kernel(key_ref, own_ref, swapped_ref, one_ref, two_ref, out_ref):
    rows, head = key_ref.shape
    total = 0.0
    for ref in (own_ref, swapped_ref, one_ref, two_ref):
        total = total + ref[...].astype(F32).reshape(rows, 2 * head)
    key = key_ref[...].astype(F32)
    scale = lax.rsqrt(jnp.mean(key * key, axis=1, keepdims=True) + NORM_FLOOR)
    hat = total[:, :head]
    grad = scale * hat - scale * scale * scale * key * jnp.mean(key * hat, axis=1, keepdims=True)
    out_ref[:, :head] = grad.astype(BF)
    out_ref[:, head:] = total[:, head:].astype(BF)


def heads_sum(pieces, weights, columns):
    total = 0.0
    for piece, rows in zip(pieces, weights):
        term = lax.dot_general(
            piece, rows[:, columns[0] : columns[1]], CONTRACT_LAST, preferred_element_type=F32
        )
        total = total + term.astype(BF).astype(F32)
    return total.astype(BF)


def token_kernel(columns, own_ref, up_ref, fa_ref, fb_ref, down_ref, *refs):
    far = jnp.concatenate([fa_ref[...], fb_ref[...]], axis=0)
    pieces = (own_ref[...], up_ref[...], down_ref[...], far)
    refs[4][...] = heads_sum(pieces, refs[:4], columns)


def store_kernel(columns, *refs):
    weights, out_ref = refs[8:12], refs[12]
    for half in range(2):

        @pl.when(pl.program_id(0) == half)
        def _():
            pieces = tuple(ref[...] for ref in refs[4 * half : 4 * half + 4])
            out_ref[...] = heads_sum(pieces, weights, columns)


def ring4(value, axis):
    half = value.shape[0] // 2
    below = shift(value, axis, 1)
    above = shift(value, axis, -1)
    far_a = shift(below[:half], axis, 1)
    far_b = shift(above[half:], axis, -1)
    return value, above, far_a, far_b, below


def ring8(value, axis):
    half = value.shape[0] // 2
    below, above = [value], [value]
    for _ in range(3):
        below.append(shift(below[-1], axis, 1))
        above.append(shift(above[-1], axis, -1))
    far_a = shift(below[3][:half], axis, 1)
    far_b = shift(above[3][half:], axis, -1)
    return [value, above[1], above[2], above[3], far_a, below[3], below[2], below[1], far_b]


def swap(value):
    return lax.ppermute(value, "c", [(0, 1), (1, 0)])


def copy_for_each(shard, axis):
    copies = jnp.broadcast_to(shard, (lax.axis_size(axis), *shard.shape))
    return lax.all_to_all(copies, axis, split_axis=0, concat_axis=0, tiled=True)


def body(
    tokens,
    cotangent,
    mix_query,
    mix_key,
    mix_value,
    beta_pre,
    decay_pre,
    decay_rate,
    passages,
    passage_ids,
    query_weight,
    key_weight,
    value_weight,
    gate_weight,
):
    tok_rows = tokens.shape[0]
    width, head = query_weight.shape
    per_owner, rows_each = passages.shape[:2]
    blocks_n, per_block = passage_ids.shape
    span = tok_rows // blocks_n
    scale = SCORE_GAIN * head ** (-0.5)
    z, y, c, x = (lax.axis_index(a) for a in ("z", "y", "c", "x"))
    slice_w = width // 4

    pos = jnp.stack([z, y, c]).astype(jnp.int32)

    tok_own, tok_up, tok_far_a, tok_far_b, tok_down = ring4(tokens, "x")
    flat_ids = passage_ids.reshape(1, -1)
    digits = jnp.concatenate([flat_ids // 32, flat_ids % 32], axis=0).astype(BF)
    digits = jnp.pad(digits, ((0, 14), (0, head - digits.shape[1])))
    column = copy_for_each(jnp.concatenate([cotangent, digits], axis=0), "z")
    got = column[:, tok_rows : tok_rows + 2, : blocks_n * per_block].astype(jnp.int32)
    ids = (got[:, 0] * 32 + got[:, 1]).reshape(-1)

    flat_rows = passages.reshape(per_owner * rows_each, width)
    key_low = lax.optimization_barrier(
        jnp.dot(flat_rows, key_weight, preferred_element_type=F32).astype(BF)
    )
    value_all = jnp.dot(flat_rows, value_weight, preferred_element_type=F32).astype(BF)
    key_float = key_low.astype(F32)
    key_scale = lax.rsqrt(jnp.mean(key_float * key_float, axis=-1, keepdims=True) + NORM_FLOOR)
    key_hat = (key_float * key_scale).astype(BF)
    packed = jnp.concatenate([key_hat, value_all], axis=-1).reshape(per_owner, rows_each, 2 * head)
    kv_pieces = ring4(packed, "y")
    kv_pieces = tuple(kv_pieces) + tuple(swap(piece) for piece in kv_pieces)

    wq_turned = lax.dynamic_slice_in_dim(
        jnp.concatenate([query_weight, query_weight], axis=0), x * slice_w, width, 0
    )
    gw_turned = lax.dynamic_slice_in_dim(
        jnp.concatenate([gate_weight, gate_weight], axis=1), x * slice_w, width, 1
    )
    tok_far = jnp.concatenate([tok_far_a, tok_far_b], axis=0)
    query_acc = 0.0
    gate_acc = 0.0
    for n, piece in enumerate((tok_own, tok_up, tok_far, tok_down)):
        query_acc = query_acc + jnp.dot(
            piece, wq_turned[n * slice_w : (n + 1) * slice_w], preferred_element_type=F32
        )
        gate_acc = gate_acc + jnp.sum(
            piece.astype(F32) * gw_turned[:, n * slice_w : (n + 1) * slice_w].astype(F32), axis=1
        )
    query_low = lax.optimization_barrier(query_acc.astype(BF))
    query_float = query_low.astype(F32)
    query_scale = lax.rsqrt(
        jnp.mean(query_float * query_float, axis=-1, keepdims=True) + NORM_FLOOR
    )
    query_hat = (query_float * query_scale).astype(BF)
    gate_open = jax.nn.sigmoid(gate_acc)
    q_pieces = ring8(query_hat, "z")

    gate_column = jnp.pad(
        jnp.broadcast_to(gate_weight.reshape(width, 1), (width, 2)), ((0, 0), (0, 126))
    )
    weights = jnp.concatenate([key_weight, value_weight, query_weight, gate_column], axis=1)
    weights, _ = lax.optimization_barrier((weights, tok_far))
    weights = weights.reshape(4, slice_w, weights.shape[1])

    def weight_rows(step):
        rows = lax.dynamic_index_in_dim(weights, (x + step) & 3, 0, keepdims=False)
        return rows if step == 0 else shift(rows, "x", step)

    weights = [weight_rows(step) for step in (0, -1, 1, 2)]

    any_space = pl.BlockSpec(memory_space=pl.ANY)
    smem = pl.BlockSpec(memory_space=pltpu.SMEM)
    vmem = pl.BlockSpec(memory_space=pltpu.VMEM)
    stores = [
        pltpu.VMEM((8, tok_rows, head), BF),
        pltpu.VMEM((8, tok_rows, head), BF),
        pltpu.VMEM((8 * per_owner, rows_each, 2 * head), BF),
    ]
    pieces = (*q_pieces, column, *kv_pieces)
    params = pltpu.CompilerParams(vmem_limit_bytes=60 * 1024 * 1024)
    message, codes, count = pl.pallas_call(
        functools.partial(sums_kernel, scale),
        out_shape=[
            jax.ShapeDtypeStruct((8, 9 * blocks_n, 2 * span), F32),
            jax.ShapeDtypeStruct((72,), jnp.int32),
            jax.ShapeDtypeStruct((1,), jnp.int32),
        ],
        in_specs=[smem, smem, vmem] + [any_space] * 20,
        out_specs=[vmem, smem, smem],
        scratch_shapes=stores + [pltpu.SemaphoreType.DMA((20,))],
        compiler_params=params,
        name="sums",
    )(ids, pos, gate_open.reshape(blocks_n, span), *pieces)
    arrived = lax.all_to_all(message, "z", split_axis=0, concat_axis=0, tiled=True)

    def part_shape(owners):
        return jax.ShapeDtypeStruct((owners * per_owner, rows_each, 2 * head), BF)

    mine_far, mine_rest, other_far, other_rest, q_parts, totals = pl.pallas_call(
        functools.partial(terms_kernel, scale),
        out_shape=[
            part_shape(1),
            part_shape(3),
            part_shape(1),
            part_shape(3),
            jax.ShapeDtypeStruct((8, tok_rows, head), BF),
            jax.ShapeDtypeStruct((8 * blocks_n, 2 * span), F32),
        ],
        in_specs=[smem, smem, smem, vmem] + [any_space] * 20,
        out_specs=[any_space] * 4 + [vmem, vmem],
        scratch_shapes=stores
        + [
            pltpu.VMEM((8 * per_owner, rows_each, 2 * head), BF),
            pltpu.VMEM((8, tok_rows, head), F32),
            pltpu.VMEM((8 * blocks_n, 2 * span), F32),
            pltpu.SemaphoreType.DMA((20,)),
        ],
        compiler_params=params,
        name="terms",
    )(codes, count, pos, arrived, *pieces)

    def plus(a, b):
        return (a.astype(F32) + b.astype(F32)).astype(BF)

    got_far = swap(other_far)
    got_rest = swap(other_rest)
    half = per_owner // 2
    got_a = shift(plus(mine_far[:half], got_far[:half]), "y", 1)
    got_b = shift(plus(mine_far[half:], got_far[half:]), "y", -1)
    near, back = 2 * per_owner, 0
    near_a, near_b, back_a, back_b = lax.optimization_barrier(
        tuple(
            plus(mine_rest[at : at + half], got_rest[at : at + half])
            for at in (near, near + half, back, back + half)
        )
    )
    early_b = shift(near_b, "y", 1)
    early_a = shift(back_a, "y", -1)
    late_a = shift(plus(near_a, got_a), "y", 1)
    late_b = shift(plus(back_b, got_b), "y", -1)

    q_back = lax.all_to_all(q_parts, "z", split_axis=0, concat_axis=0, tiled=True)
    qhat_grad = jnp.sum(q_back.astype(F32), axis=0)
    query_grad = (
        query_scale * qhat_grad
        - query_scale**3 * query_float * jnp.mean(query_float * qhat_grad, axis=-1, keepdims=True)
    ).astype(BF)
    mix_query, _ = lax.optimization_barrier((mix_query, q_parts))
    mixed_dot = mixer_dot(
        mix_query, mix_key, mix_value, cotangent, beta_pre, decay_pre, decay_rate
    ).reshape(tok_rows)
    own_totals = lax.dynamic_slice_in_dim(totals, z * blocks_n, blocks_n, 0)
    retrieved_dot = own_totals[:, span:].reshape(tok_rows)
    gate_grad = (retrieved_dot - mixed_dot) * gate_open * (1.0 - gate_open)
    high = gate_grad.astype(BF)
    rest = (gate_grad - high.astype(F32)).astype(BF)
    columns = jnp.pad(jnp.stack([high, rest], axis=1), ((0, 0), (0, 126)))
    token_pieces = ring4(jnp.concatenate([query_grad, columns], axis=1), "x")
    token_grad = pl.pallas_call(
        functools.partial(token_kernel, (2 * head, 3 * head + 128)),
        out_shape=jax.ShapeDtypeStruct((tok_rows, slice_w), BF),
        in_specs=[vmem] * 9,
        out_specs=vmem,
        compiler_params=params,
        name="token_rows",
    )(*token_pieces, *weights)

    half_rows = half * rows_each
    steps = 2
    tile = (half // steps, rows_each, 2 * head)
    tile_rows = half_rows // steps
    grads = []
    for n, one, two in ((0, early_a, late_a), (1, early_b, late_b)):
        own_part = pl.BlockSpec(tile, lambda i, n=n: (i + (2 + n) * steps, 0, 0))
        sent = pl.BlockSpec(tile, lambda i: (i, 0, 0))
        grads.append(
            pl.pallas_call(
                finish_kernel,
                grid=(steps,),
                out_shape=jax.ShapeDtypeStruct((half_rows, 2 * head), BF),
                in_specs=[
                    pl.BlockSpec((tile_rows, head), lambda i, n=n: (i + n * steps, 0)),
                    own_part,
                    own_part,
                    sent,
                    sent,
                ],
                out_specs=pl.BlockSpec((tile_rows, 2 * head), lambda i: (i, 0)),
                compiler_params=params,
            )(key_low, mine_rest, got_rest, one, two)
        )
    up_b = shift(grads[1], "x", -1)
    down_a = shift(grads[0], "x", 1)
    down_b, up_a = shift(grads[1], "x", 1), shift(grads[0], "x", -1)
    far_a, far_b = shift(down_a, "x", 1), shift(up_b, "x", -1)
    weight_b = lax.optimization_barrier(
        lax.dot_general(
            flat_rows[half_rows:], grads[1][:, :head], CONTRACT_FIRST, preferred_element_type=F32
        )
    )
    weight_term = (
        weight_b
        + lax.dot_general(
            flat_rows[:half_rows], grads[0][:, :head], CONTRACT_FIRST, preferred_element_type=F32
        )
    ).astype(BF)
    weight_back = lax.all_to_all(
        weight_term.reshape(64, width // 64, head), ST, split_axis=0, concat_axis=0, tiled=True
    )
    key_weight_grad = jnp.sum(weight_back.astype(F32), axis=0)
    passage_grad = pl.pallas_call(
        functools.partial(store_kernel, (0, 2 * head)),
        grid=(2,),
        out_shape=jax.ShapeDtypeStruct((per_owner * rows_each, slice_w), BF),
        in_specs=[pl.BlockSpec((half_rows, 2 * head), lambda i: (0, 0))] * 8
        + [pl.BlockSpec((slice_w, 2 * head), lambda i: (0, 0))] * 4,
        out_specs=pl.BlockSpec((half_rows, slice_w), lambda i: (i, 0)),
        compiler_params=params,
        name="store_rows",
    )(grads[0], up_a, down_a, far_a, grads[1], up_b, down_b, far_b, *weights).reshape(
        per_owner, rows_each, slice_w
    )
    return (token_grad, passage_grad, key_weight_grad)


def solution(mesh):
    torus = Mesh(mesh.devices.reshape(8, 4, 2, mesh.shape["tp"]), ("z", "y", "c", "x"))

    return jax.shard_map(
        body,
        mesh=torus,
        in_specs=(
            P(ST, "x"),
            P(ST, "x"),
            P(ST, "x"),
            P(ST, "x"),
            P(ST, "x"),
            P("x", ST),
            P("x", ST),
            P("x"),
            P(ST, None, None),
            P(ST, None),
            P(None, "x"),
            P(None, "x"),
            P(None, "x"),
            P("x", None),
        ),
        out_specs=(P(ST, "x"), P(ST, None, "x"), P(ST, "x")),
        check_vma=False,
    )
```

```python
import functools

import jax
import jax.numpy as jnp
from jax import lax
from jax.experimental import pallas as pl
from jax.experimental.pallas import tpu as pltpu
from jax.sharding import Mesh
from jax.sharding import PartitionSpec as P


SPAN = 64
ST = ("z", "y", "c")
NORM_FLOOR = 1.0
SCORE_GAIN = 4.0
CONTRACT_LAST = (((1,), (1,)), ((), ()))
CONTRACT_FIRST = (((0,), (0,)), ((), ()))
BF = jnp.bfloat16
F32 = jnp.float32


def shift(value, axis, step):
    n = lax.axis_size(axis)
    return lax.ppermute(value, axis, [(i, (i + step) % n) for i in range(n)])


def low_dot(a, b, dims=(((1,), (0,)), ((), ()))):
    return lax.dot_general(a.astype(BF), b.astype(BF), dims, preferred_element_type=F32)


def mixer_kernel(q_ref, k_ref, v_ref, cot_ref, rows_ref, cols_ref, out_ref):
    length, width = q_ref.shape
    heads_n = 2
    dim = width // heads_n
    blocks_n = length // SPAN
    at = lax.broadcasted_iota(jnp.int32, (SPAN, SPAN), 0)
    to = lax.broadcasted_iota(jnp.int32, (SPAN, SPAN), 1)
    eye = (at == to).astype(F32)
    pairs = [(h, n) for n in range(blocks_n) for h in range(heads_n)]
    held = {}
    for h, n in pairs:
        part = (slice(n * SPAN, (n + 1) * SPAN), slice(h * dim, (h + 1) * dim))
        q, k, v = (ref[part].astype(F32) for ref in (q_ref, k_ref, v_ref))
        q = q * lax.rsqrt(jnp.sum(q * q, axis=1, keepdims=True) + NORM_FLOOR) * dim ** (-0.5)
        k = k * lax.rsqrt(jnp.sum(k * k, axis=1, keepdims=True) + NORM_FLOOR)
        m = h * blocks_n + n
        cum_row = rows_ref[m : m + 1, :]
        cum = cols_ref[:, m : m + 1]
        strength = cols_ref[:, 2 * blocks_n + m : 2 * blocks_n + m + 1]
        last = rows_ref[m : m + 1, SPAN - 1 : SPAN]
        decay = jnp.exp(jnp.where(at >= to, cum - cum_row, -jnp.inf))
        grow = jnp.exp(cum)
        strict = jnp.where(at > to, strength * low_dot(k, k, CONTRACT_LAST) * decay, 0.0)
        attend = jnp.where(at >= to, low_dot(q, k, CONTRACT_LAST) * decay, 0.0).astype(BF)
        right = jnp.concatenate([v * strength, k * (strength * grow)], axis=1).astype(BF)
        held[h, n] = [
            strict,
            right,
            attend,
            (q * grow).astype(BF),
            (k * jnp.exp(last - cum)).astype(BF),
            jnp.exp(last),
        ]
    running = {p: eye - held[p][0] for p in pairs}
    power = {p: held[p][0] for p in pairs}
    for _ in range(SPAN.bit_length() - 2):
        for p in pairs:
            power[p] = low_dot(power[p], power[p])
        for p in pairs:
            running[p] = low_dot(running[p], eye + power[p])
    solved = {p: low_dot(running[p], held[p][1]) for p in pairs}
    state = [jnp.zeros((dim, dim), F32) for _ in range(heads_n)]
    for n in range(blocks_n):
        rows = slice(n * SPAN, (n + 1) * SPAN)
        total = 0.0
        for h in range(heads_n):
            _, _, attend, q_dec, k_dec, carry = held[h, n]
            s_low = state[h].astype(BF)
            fresh = (solved[h, n][:, :dim] - low_dot(solved[h, n][:, dim:], s_low)).astype(BF)
            out = low_dot(q_dec, s_low) + low_dot(attend, fresh)
            state[h] = state[h] * carry + low_dot(k_dec, fresh, CONTRACT_FIRST)
            cot = cot_ref[rows, h * dim : (h + 1) * dim].astype(F32)
            total = total + jnp.sum(out * cot, axis=1, keepdims=True)
        out_ref[rows, :] = total


def mixer_dot(query_raw, key_raw, value_raw, cotangent, beta_raw, decay_raw, rate_vals):
    strength = jax.nn.sigmoid(beta_raw).reshape(-1, SPAN)
    log_decay = (-rate_vals[:, None] * jax.nn.softplus(decay_raw)).reshape(-1, SPAN)
    upto = (jnp.arange(SPAN)[:, None] <= jnp.arange(SPAN)[None, :]).astype(F32)
    cumulative = jnp.dot(log_decay, upto, precision=lax.Precision.HIGHEST)
    columns = jnp.concatenate([cumulative, strength], axis=0).T
    vmem = pl.BlockSpec(memory_space=pltpu.VMEM)
    return pl.pallas_call(
        mixer_kernel,
        out_shape=jax.ShapeDtypeStruct((query_raw.shape[0], 1), F32),
        in_specs=[vmem] * 6,
        out_specs=vmem,
        name="mixer",
    )(query_raw, key_raw, value_raw, cotangent, cumulative, columns)


def fetch(pos_ref, q_refs, kv_refs, qs, kvs, sems):
    z, y = pos_ref[0], pos_ref[1]
    rows = qs.shape[1]
    per = kvs.shape[0] // 8
    copies = []

    def add(src, dst):
        copies.append(pltpu.make_async_copy(src, dst, sems.at[len(copies)]))

    for rel in range(8):
        slot = (z + rel) & 7
        if rel == 4:
            add(q_refs[4], qs.at[slot, pl.ds(0, rows // 2)])
            add(q_refs[8], qs.at[slot, pl.ds(rows // 2, rows // 2)])
        else:
            add(q_refs[rel], qs.at[slot])
    for other, ref in enumerate(kv_refs):
        for rel in range(4):
            add(ref.at[(y + rel) & 3], kvs.at[pl.ds((other * 4 + ((rel + 2) & 3)) * per, per)])
    for copy in copies:
        copy.start()
    return copies


def split_code(code):
    row = code >> 7
    return row, row // 6, row % 6, code & 127


def pair_scores(scale, q, cot, kv):
    head = q.shape[-1]
    scores = lax.dot_general(kv[:, :head], q, CONTRACT_LAST, preferred_element_type=F32) * scale
    grads = lax.dot_general(kv[:, head:], cot, CONTRACT_LAST, preferred_element_type=F32)
    return jnp.exp(scores), grads


def sums_kernel(scale, requests, pos_ref, gate_ref, *refs):
    q_refs, kv_refs = refs[:9], refs[9:11]
    out_ref, code_ref, count_ref, qs, kvs, ids_vmem, ids_ref, sems = refs[11:]
    copies = fetch(pos_ref, q_refs, kv_refs, qs, kvs, sems)
    blocks_n, span = gate_ref.shape
    blocks_all = 8 * blocks_n
    out_ref[...] = jnp.zeros_like(out_ref)
    z, y, c = pos_ref[0], pos_ref[1], pos_ref[2]
    per_owner = kvs.shape[0] // 8
    per_block = requests // blocks_n
    tok_rows = blocks_n * span
    head = qs.shape[2] // 2

    def clear(i, carry):
        code_ref[i] = 0
        return carry

    lax.fori_loop(0, code_ref.shape[0], clear, 0)

    for copy in copies:
        copy.wait()
    digits = qs[:, tok_rows : tok_rows + 16, :128].astype(F32)
    ids_vmem[...] = (digits[:, 0, :] * 32.0 + digits[:, 1, :]).astype(jnp.int32)
    to_scalars = pltpu.make_async_copy(ids_vmem, ids_ref, sems.at[len(copies)])
    to_scalars.start()
    to_scalars.wait()

    def collect(row, found):
        for j in range(per_block):
            one = ids_ref[row // blocks_n, row % blocks_n * per_block + j]
            lane = (one // per_owner) & 7
            place = ((lane & 1) ^ c) * 4 + (((lane >> 1) - y + 2) & 3)
            code_ref[found] = row * 128 + place * per_owner + one % per_owner
            found = found + (one // (8 * per_owner) == z).astype(jnp.int32)
        return found

    count = lax.fori_loop(0, blocks_all, collect, jnp.int32(0))
    code_ref[count] = 0
    count_ref[0] = count

    def step(i, carry):
        done = []
        for u in range(2):
            at = 2 * i + u
            row, reader, block, slot = split_code(code_ref[at])
            tok = pl.ds(pl.multiple_of(block * span, span), span)
            both = qs[reader, tok]
            e, g = pair_scores(scale, both[:, :head], both[:, head:], kvs[slot])
            both = jnp.concatenate(
                [jnp.sum(e, axis=0, keepdims=True), jnp.sum(e * g, axis=0, keepdims=True)], axis=1
            )
            done.append((row, jnp.where(at < count, both, 0.0)))
        for row, both in done:
            out_ref[0, pl.ds(row, 1), :] += both
        return carry

    lax.fori_loop(0, (count + 1) // 2, step, 0)
    out_ref[0, blocks_all : blocks_all + blocks_n, 0:span] = gate_ref[...]
    for i in range(1, 8):
        out_ref[i] = out_ref[0]


def terms_kernel(scale, code_ref, count_ref, pos_ref, arrived_ref, *refs):
    q_refs, kv_refs = refs[:9], refs[9:11]
    part_refs, qout_ref, tot_ref = refs[11:15], refs[15], refs[16]
    qs, kvs, acc, qacc, gates, sems = refs[17:]
    copies = fetch(pos_ref, q_refs, kv_refs, qs, kvs, sems)
    head = qs.shape[2] // 2
    acc[...] = jnp.zeros_like(acc)
    qacc[...] = jnp.zeros_like(qacc)
    count = count_ref[0]
    blocks_all = tot_ref.shape[0]
    span = tot_ref.shape[1] // 2
    blocks_n = blocks_all // 8
    summed = jnp.sum(arrived_ref[:, :blocks_all, :], axis=0)
    lanes = lax.broadcasted_iota(jnp.int32, summed.shape, 1)
    weights = jnp.concatenate([summed[:, :span], summed[:, :span]], axis=1)
    tot_ref[...] = jnp.where(lanes < span, summed, summed / weights)
    for i in range(8):
        gates[i * blocks_n : (i + 1) * blocks_n, :] = arrived_ref[
            i, blocks_all : blocks_all + blocks_n, :
        ]
    for copy in copies:
        copy.wait()

    def step(i, carry):
        done = []
        for u in range(2):
            at = 2 * i + u
            row, reader, block, slot = split_code(code_ref[at])
            tok = pl.ds(pl.multiple_of(block * span, span), span)
            both, kv = qs[reader, tok], kvs[slot]
            q, cot = both[:, :head], both[:, head:]
            e, g = pair_scores(scale, q, cot, kv)
            tot = tot_ref[pl.ds(row, 1), :]
            gated = e * (gates[pl.ds(row, 1), :][:, :span] / tot[:, :span])
            low = gated.astype(BF)
            grad = (gated * (g - tot[:, span:])).astype(BF)
            key_term = lax.dot_general(
                grad, q, (((1,), (0,)), ((), ())), preferred_element_type=F32
            ) * scale
            value_term = lax.dot_general(
                low, cot, (((1,), (0,)), ((), ())), preferred_element_type=F32
            )
            q_term = lax.dot_general(
                grad, kv[:, : q.shape[-1]], CONTRACT_FIRST, preferred_element_type=F32
            ) * scale
            both = jnp.concatenate([key_term, value_term], axis=1).astype(BF).astype(F32)
            valid = at < count
            done.append((slot, reader, tok, jnp.where(valid, both, 0.0), jnp.where(valid, q_term, 0.0)))
        for slot, reader, tok, both, q_term in done:
            acc[slot] = (acc[slot].astype(F32) + both).astype(BF)
            qacc[reader, tok] += q_term
        return carry

    lax.fori_loop(0, (count + 1) // 2, step, 0)
    outs = []
    order = (2, 0, 3, 1)
    starts = {0: 0, 1: part_refs[0].shape[0]}
    starts[2] = starts[1] + part_refs[1].shape[0]
    starts[3] = starts[2] + part_refs[2].shape[0]
    for n in order:
        ref = part_refs[n]
        copy = pltpu.make_async_copy(acc.at[pl.ds(starts[n], ref.shape[0])], ref, sems.at[n])
        copy.start()
        outs.append(copy)
    qout_ref[...] = qacc[...].astype(BF)
    for copy in outs:
        copy.wait()


def finish_kernel(key_ref, own_ref, swapped_ref, one_ref, two_ref, out_ref):
    rows, head = key_ref.shape
    total = 0.0
    for ref in (own_ref, swapped_ref, one_ref, two_ref):
        total = total + ref[...].astype(F32).reshape(rows, 2 * head)
    key = key_ref[...].astype(F32)
    scale = lax.rsqrt(jnp.mean(key * key, axis=1, keepdims=True) + NORM_FLOOR)
    hat = total[:, :head]
    grad = scale * hat - scale * scale * scale * key * jnp.mean(key * hat, axis=1, keepdims=True)
    out_ref[:, :head] = grad.astype(BF)
    out_ref[:, head:] = total[:, head:].astype(BF)


def heads_sum(pieces, weights, columns):
    total = 0.0
    for piece, rows in zip(pieces, weights):
        term = lax.dot_general(
            piece, rows[:, columns[0] : columns[1]], CONTRACT_LAST, preferred_element_type=F32
        )
        total = total + term.astype(BF).astype(F32)
    return total.astype(BF)


def token_kernel(columns, *refs):
    refs[8][...] = heads_sum(tuple(ref[...] for ref in refs[:4]), refs[4:8], columns)


def store_kernel(columns, *refs):
    weights, out_ref = refs[8:12], refs[12]
    for half in range(2):

        @pl.when(pl.program_id(0) == half)
        def _():
            pieces = tuple(ref[...] for ref in refs[4 * half : 4 * half + 4])
            out_ref[...] = heads_sum(pieces, weights, columns)


def all4(value, axis):
    return value, shift(value, axis, -1), shift(value, axis, 1), shift(value, axis, 2)


def ring8(value, axis):
    half = value.shape[0] // 2
    below, above = [value], [value]
    for _ in range(3):
        below.append(shift(below[-1], axis, 1))
        above.append(shift(above[-1], axis, -1))
    far_a = shift(below[3][:half], axis, 1)
    far_b = shift(above[3][half:], axis, -1)
    return [value, above[1], above[2], above[3], far_a, below[3], below[2], below[1], far_b]


def swap(value):
    return lax.ppermute(value, "c", [(0, 1), (1, 0)])


def copy_for_each(shard, axis):
    copies = jnp.broadcast_to(shard, (lax.axis_size(axis), *shard.shape))
    return lax.all_to_all(copies, axis, split_axis=0, concat_axis=0, tiled=True)


def body(
    tokens,
    cotangent,
    mix_query,
    mix_key,
    mix_value,
    beta_pre,
    decay_pre,
    decay_rate,
    passages,
    passage_ids,
    query_weight,
    key_weight,
    value_weight,
    gate_weight,
):
    tok_rows = tokens.shape[0]
    width, head = query_weight.shape
    per_owner, rows_each = passages.shape[:2]
    blocks_n, per_block = passage_ids.shape
    span = tok_rows // blocks_n
    scale = SCORE_GAIN * head ** (-0.5)
    z, y, c, x = (lax.axis_index(a) for a in ("z", "y", "c", "x"))
    slice_w = width // 4

    pos = jnp.stack([z, y, c]).astype(jnp.int32)

    tok_pieces = all4(tokens, "x")

    flat_rows = passages.reshape(per_owner * rows_each, width)
    key_low = lax.optimization_barrier(
        jnp.dot(flat_rows, key_weight, preferred_element_type=F32).astype(BF)
    )
    value_all = jnp.dot(flat_rows, value_weight, preferred_element_type=F32).astype(BF)
    key_float = key_low.astype(F32)
    key_scale = lax.rsqrt(jnp.mean(key_float * key_float, axis=-1, keepdims=True) + NORM_FLOOR)
    key_hat = (key_float * key_scale).astype(BF)
    packed = jnp.concatenate([key_hat, value_all], axis=-1).reshape(per_owner, rows_each, 2 * head)
    kv_own = copy_for_each(packed[None], "y").reshape(4, *packed.shape)
    kv_other = swap(kv_own)

    wq_turned = lax.dynamic_slice_in_dim(
        jnp.concatenate([query_weight, query_weight], axis=0), x * slice_w, width, 0
    )
    gw_turned = lax.dynamic_slice_in_dim(
        jnp.concatenate([gate_weight, gate_weight], axis=1), x * slice_w, width, 1
    )
    query_acc = 0.0
    gate_acc = 0.0
    for n, piece in ((0, tok_pieces[0]), (1, tok_pieces[1]), (3, tok_pieces[2]), (2, tok_pieces[3])):
        query_acc = query_acc + jnp.dot(
            piece, wq_turned[n * slice_w : (n + 1) * slice_w], preferred_element_type=F32
        )
        gate_acc = gate_acc + jnp.sum(
            piece.astype(F32) * gw_turned[:, n * slice_w : (n + 1) * slice_w].astype(F32), axis=1
        )
    query_low = lax.optimization_barrier(query_acc.astype(BF))
    query_float = query_low.astype(F32)
    query_scale = lax.rsqrt(
        jnp.mean(query_float * query_float, axis=-1, keepdims=True) + NORM_FLOOR
    )
    query_hat = (query_float * query_scale).astype(BF)
    gate_open = jax.nn.sigmoid(gate_acc)
    flat_ids = passage_ids.reshape(1, -1)
    digits = jnp.concatenate([flat_ids // 32, flat_ids % 32], axis=0).astype(BF)
    digits = jnp.pad(digits, ((0, 30), (0, 2 * head - digits.shape[1])))
    pieces = ring8(
        jnp.concatenate([jnp.concatenate([query_hat, cotangent], axis=1), digits], axis=0), "z"
    )

    gate_column = jnp.pad(
        jnp.broadcast_to(gate_weight.reshape(width, 1), (width, 2)), ((0, 0), (0, 126))
    )
    weights = jnp.concatenate([key_weight, value_weight, query_weight, gate_column], axis=1)
    weights, _ = lax.optimization_barrier((weights, tok_pieces[3]))
    weights = weights.reshape(4, slice_w, weights.shape[1])

    def weight_rows(step):
        rows = lax.dynamic_index_in_dim(weights, (x + step) & 3, 0, keepdims=False)
        return rows if step == 0 else shift(rows, "x", step)

    weights = [weight_rows(step) for step in (0, -1, 1, 2)]

    any_space = pl.BlockSpec(memory_space=pl.ANY)
    smem = pl.BlockSpec(memory_space=pltpu.SMEM)
    vmem = pl.BlockSpec(memory_space=pltpu.VMEM)
    stores = [
        pltpu.VMEM((8, *pieces[0].shape), BF),
        pltpu.VMEM((8 * per_owner, rows_each, 2 * head), BF),
    ]
    pieces = (*pieces, kv_own, kv_other)
    params = pltpu.CompilerParams(vmem_limit_bytes=60 * 1024 * 1024)
    message, codes, count = pl.pallas_call(
        functools.partial(sums_kernel, scale, blocks_n * per_block),
        out_shape=[
            jax.ShapeDtypeStruct((8, 9 * blocks_n, 2 * span), F32),
            jax.ShapeDtypeStruct((72,), jnp.int32),
            jax.ShapeDtypeStruct((1,), jnp.int32),
        ],
        in_specs=[smem, vmem] + [any_space] * 11,
        out_specs=[vmem, smem, smem],
        scratch_shapes=stores
        + [
            pltpu.VMEM((8, 128), jnp.int32),
            pltpu.SMEM((8, 128), jnp.int32),
            pltpu.SemaphoreType.DMA((18,)),
        ],
        compiler_params=params,
        name="sums",
    )(pos, gate_open.reshape(blocks_n, span), *pieces)
    arrived = lax.all_to_all(message, "z", split_axis=0, concat_axis=0, tiled=True)

    def part_shape(owners):
        return jax.ShapeDtypeStruct((owners * per_owner, rows_each, 2 * head), BF)

    mine_far, mine_rest, other_far, other_rest, q_parts, totals = pl.pallas_call(
        functools.partial(terms_kernel, scale),
        out_shape=[
            part_shape(1),
            part_shape(3),
            part_shape(1),
            part_shape(3),
            jax.ShapeDtypeStruct((8, tok_rows, head), BF),
            jax.ShapeDtypeStruct((8 * blocks_n, 2 * span), F32),
        ],
        in_specs=[smem, smem, smem, vmem] + [any_space] * 11,
        out_specs=[any_space] * 4 + [vmem, vmem],
        scratch_shapes=stores
        + [
            pltpu.VMEM((8 * per_owner, rows_each, 2 * head), BF),
            pltpu.VMEM((8, tok_rows, head), F32),
            pltpu.VMEM((8 * blocks_n, 2 * span), F32),
            pltpu.SemaphoreType.DMA((17,)),
        ],
        compiler_params=params,
        name="terms",
    )(codes, count, pos, arrived, *pieces)

    def plus(a, b):
        return (a.astype(F32) + b.astype(F32)).astype(BF)

    got_far = swap(other_far)
    got_rest = swap(other_rest)
    half = per_owner // 2
    got_a = shift(plus(mine_far[:half], got_far[:half]), "y", 1)
    got_b = shift(plus(mine_far[half:], got_far[half:]), "y", -1)
    near, back = 2 * per_owner, 0
    near_a, near_b, back_a, back_b = lax.optimization_barrier(
        tuple(
            plus(mine_rest[at : at + half], got_rest[at : at + half])
            for at in (near, near + half, back, back + half)
        )
    )
    early_b = shift(near_b, "y", 1)
    early_a = shift(back_a, "y", -1)
    late_a = shift(plus(near_a, got_a), "y", 1)
    late_b = shift(plus(back_b, got_b), "y", -1)

    q_back = lax.all_to_all(q_parts, "z", split_axis=0, concat_axis=0, tiled=True)
    qhat_grad = jnp.sum(q_back.astype(F32), axis=0)
    query_grad = (
        query_scale * qhat_grad
        - query_scale**3 * query_float * jnp.mean(query_float * qhat_grad, axis=-1, keepdims=True)
    ).astype(BF)
    mix_query, _ = lax.optimization_barrier((mix_query, q_parts))
    mixed_dot = mixer_dot(
        mix_query, mix_key, mix_value, cotangent, beta_pre, decay_pre, decay_rate
    ).reshape(tok_rows)
    own_totals = lax.dynamic_slice_in_dim(totals, z * blocks_n, blocks_n, 0)
    retrieved_dot = own_totals[:, span:].reshape(tok_rows)
    gate_grad = (retrieved_dot - mixed_dot) * gate_open * (1.0 - gate_open)
    high = gate_grad.astype(BF)
    rest = (gate_grad - high.astype(F32)).astype(BF)
    columns = jnp.pad(jnp.stack([high, rest], axis=1), ((0, 0), (0, 126)))
    token_pieces = all4(jnp.concatenate([query_grad, columns], axis=1), "x")
    token_grad = pl.pallas_call(
        functools.partial(token_kernel, (2 * head, 3 * head + 128)),
        out_shape=jax.ShapeDtypeStruct((tok_rows, slice_w), BF),
        in_specs=[vmem] * 8,
        out_specs=vmem,
        compiler_params=params,
        name="token_rows",
    )(*token_pieces, *weights)

    half_rows = half * rows_each
    steps = 2
    tile = (half // steps, rows_each, 2 * head)
    tile_rows = half_rows // steps
    grads = []
    for n, one, two in ((0, early_a, late_a), (1, early_b, late_b)):
        own_part = pl.BlockSpec(tile, lambda i, n=n: (i + (2 + n) * steps, 0, 0))
        sent = pl.BlockSpec(tile, lambda i: (i, 0, 0))
        grads.append(
            pl.pallas_call(
                finish_kernel,
                grid=(steps,),
                out_shape=jax.ShapeDtypeStruct((half_rows, 2 * head), BF),
                in_specs=[
                    pl.BlockSpec((tile_rows, head), lambda i, n=n: (i + n * steps, 0)),
                    own_part,
                    own_part,
                    sent,
                    sent,
                ],
                out_specs=pl.BlockSpec((tile_rows, 2 * head), lambda i: (i, 0)),
                compiler_params=params,
            )(key_low, mine_rest, got_rest, one, two)
        )
    up_b = shift(grads[1], "x", -1)
    down_a = shift(grads[0], "x", 1)
    down_b, up_a = shift(grads[1], "x", 1), shift(grads[0], "x", -1)
    far_a, far_b = shift(down_a, "x", 1), shift(up_b, "x", -1)
    weight_b = lax.optimization_barrier(
        lax.dot_general(
            flat_rows[half_rows:], grads[1][:, :head], CONTRACT_FIRST, preferred_element_type=F32
        )
    )
    weight_term = (
        weight_b
        + lax.dot_general(
            flat_rows[:half_rows], grads[0][:, :head], CONTRACT_FIRST, preferred_element_type=F32
        )
    ).astype(BF)
    weight_term = weight_term.reshape(32, 2, width // 64, head)
    weight_other = swap(lax.dynamic_index_in_dim(weight_term, c ^ 1, 1, keepdims=False))
    weight_mine = plus(lax.dynamic_index_in_dim(weight_term, c, 1, keepdims=False), weight_other)
    weight_back = lax.all_to_all(weight_mine, ("z", "y"), split_axis=0, concat_axis=0, tiled=True)
    key_weight_grad = jnp.sum(weight_back.astype(F32), axis=0)
    passage_grad = pl.pallas_call(
        functools.partial(store_kernel, (0, 2 * head)),
        grid=(2,),
        out_shape=jax.ShapeDtypeStruct((per_owner * rows_each, slice_w), BF),
        in_specs=[pl.BlockSpec((half_rows, 2 * head), lambda i: (0, 0))] * 8
        + [pl.BlockSpec((slice_w, 2 * head), lambda i: (0, 0))] * 4,
        out_specs=pl.BlockSpec((half_rows, slice_w), lambda i: (i, 0)),
        compiler_params=params,
        name="store_rows",
    )(grads[0], up_a, down_a, far_a, grads[1], up_b, down_b, far_b, *weights).reshape(
        per_owner, rows_each, slice_w
    )
    return (token_grad, passage_grad, key_weight_grad)


def solution(mesh):
    torus = Mesh(mesh.devices.reshape(8, 4, 2, mesh.shape["tp"]), ("z", "y", "c", "x"))

    return jax.shard_map(
        body,
        mesh=torus,
        in_specs=(
            P(ST, "x"),
            P(ST, "x"),
            P(ST, "x"),
            P(ST, "x"),
            P(ST, "x"),
            P("x", ST),
            P("x", ST),
            P("x"),
            P(ST, None, None),
            P(ST, None),
            P(None, "x"),
            P(None, "x"),
            P(None, "x"),
            P("x", None),
        ),
        out_specs=(P(ST, "x"), P(ST, None, "x"), P(ST, "x")),
        check_vma=False,
    )
```

```python
import functools

import jax
import jax.numpy as jnp
from jax import lax
from jax.experimental import pallas as pl
from jax.experimental.pallas import tpu as pltpu
from jax.sharding import Mesh
from jax.sharding import PartitionSpec as P


SPAN = 64
ST = ("z", "y", "c")
NORM_FLOOR = 1.0
SCORE_GAIN = 4.0
CONTRACT_LAST = (((1,), (1,)), ((), ()))
CONTRACT_FIRST = (((0,), (0,)), ((), ()))
BF = jnp.bfloat16
F32 = jnp.float32


def shift(value, axis, step):
    n = lax.axis_size(axis)
    return lax.ppermute(value, axis, [(i, (i + step) % n) for i in range(n)])


def low_dot(a, b, dims=(((1,), (0,)), ((), ()))):
    return lax.dot_general(a.astype(BF), b.astype(BF), dims, preferred_element_type=F32)


def mixer_kernel(q_ref, k_ref, v_ref, cot_ref, rows_ref, cols_ref, out_ref):
    length, width = q_ref.shape
    heads_n = 2
    dim = width // heads_n
    blocks_n = length // SPAN
    at = lax.broadcasted_iota(jnp.int32, (SPAN, SPAN), 0)
    to = lax.broadcasted_iota(jnp.int32, (SPAN, SPAN), 1)
    eye = (at == to).astype(F32)
    pairs = [(h, n) for n in range(blocks_n) for h in range(heads_n)]
    held = {}
    for h, n in pairs:
        part = (slice(n * SPAN, (n + 1) * SPAN), slice(h * dim, (h + 1) * dim))
        q, k, v = (ref[part].astype(F32) for ref in (q_ref, k_ref, v_ref))
        q = q * lax.rsqrt(jnp.sum(q * q, axis=1, keepdims=True) + NORM_FLOOR) * dim ** (-0.5)
        k = k * lax.rsqrt(jnp.sum(k * k, axis=1, keepdims=True) + NORM_FLOOR)
        m = h * blocks_n + n
        cum_row = rows_ref[m : m + 1, :]
        cum = cols_ref[:, m : m + 1]
        strength = cols_ref[:, 2 * blocks_n + m : 2 * blocks_n + m + 1]
        last = rows_ref[m : m + 1, SPAN - 1 : SPAN]
        decay = jnp.exp(jnp.where(at >= to, cum - cum_row, -jnp.inf))
        grow = jnp.exp(cum)
        strict = jnp.where(at > to, strength * low_dot(k, k, CONTRACT_LAST) * decay, 0.0)
        attend = jnp.where(at >= to, low_dot(q, k, CONTRACT_LAST) * decay, 0.0).astype(BF)
        right = jnp.concatenate([v * strength, k * (strength * grow)], axis=1).astype(BF)
        held[h, n] = [
            strict,
            right,
            attend,
            (q * grow).astype(BF),
            (k * jnp.exp(last - cum)).astype(BF),
            jnp.exp(last),
        ]
    running = {p: eye - held[p][0] for p in pairs}
    power = {p: held[p][0] for p in pairs}
    for _ in range(SPAN.bit_length() - 2):
        for p in pairs:
            power[p] = low_dot(power[p], power[p])
        for p in pairs:
            running[p] = low_dot(running[p], eye + power[p])
    solved = {p: low_dot(running[p], held[p][1]) for p in pairs}
    state = [jnp.zeros((dim, dim), F32) for _ in range(heads_n)]
    for n in range(blocks_n):
        rows = slice(n * SPAN, (n + 1) * SPAN)
        total = 0.0
        for h in range(heads_n):
            _, _, attend, q_dec, k_dec, carry = held[h, n]
            s_low = state[h].astype(BF)
            fresh = (solved[h, n][:, :dim] - low_dot(solved[h, n][:, dim:], s_low)).astype(BF)
            out = low_dot(q_dec, s_low) + low_dot(attend, fresh)
            state[h] = state[h] * carry + low_dot(k_dec, fresh, CONTRACT_FIRST)
            cot = cot_ref[rows, h * dim : (h + 1) * dim].astype(F32)
            total = total + jnp.sum(out * cot, axis=1, keepdims=True)
        out_ref[rows, :] = total


def mixer_dot(query_raw, key_raw, value_raw, cotangent, beta_raw, decay_raw, rate_vals):
    strength = jax.nn.sigmoid(beta_raw).reshape(-1, SPAN)
    log_decay = (-rate_vals[:, None] * jax.nn.softplus(decay_raw)).reshape(-1, SPAN)
    upto = (jnp.arange(SPAN)[:, None] <= jnp.arange(SPAN)[None, :]).astype(F32)
    cumulative = jnp.dot(log_decay, upto, precision=lax.Precision.HIGHEST)
    columns = jnp.concatenate([cumulative, strength], axis=0).T
    vmem = pl.BlockSpec(memory_space=pltpu.VMEM)
    return pl.pallas_call(
        mixer_kernel,
        out_shape=jax.ShapeDtypeStruct((query_raw.shape[0], 1), F32),
        in_specs=[vmem] * 6,
        out_specs=vmem,
        name="mixer",
    )(query_raw, key_raw, value_raw, cotangent, cumulative, columns)


def fetch(pos_ref, q_refs, kv_refs, qs, kvs, sems):
    z, y = pos_ref[0], pos_ref[1]
    rows = qs.shape[1]
    per = kvs.shape[0] // 8
    copies = []

    def add(src, dst):
        copies.append(pltpu.make_async_copy(src, dst, sems.at[len(copies)]))

    for rel in range(8):
        slot = (z + rel) & 7
        if rel == 4:
            add(q_refs[4], qs.at[slot, pl.ds(0, rows // 2)])
            add(q_refs[8], qs.at[slot, pl.ds(rows // 2, rows // 2)])
        else:
            add(q_refs[rel], qs.at[slot])
    for other, ref in enumerate(kv_refs):
        for rel in range(4):
            add(ref.at[(y + rel) & 3], kvs.at[pl.ds((other * 4 + ((rel + 2) & 3)) * per, per)])
    for copy in copies:
        copy.start()
    return copies


def split_code(code):
    row = code >> 7
    return row, row // 6, row % 6, code & 127


def pair_scores(scale, q, cot, kv):
    head = q.shape[-1]
    scores = lax.dot_general(kv[:, :head], q, CONTRACT_LAST, preferred_element_type=F32) * scale
    grads = lax.dot_general(kv[:, head:], cot, CONTRACT_LAST, preferred_element_type=F32)
    return jnp.exp(scores), grads


def sums_kernel(scale, requests, pos_ref, gate_ref, *refs):
    q_refs, kv_refs = refs[:9], refs[9:11]
    out_ref, code_ref, count_ref, qs, kvs, ids_vmem, ids_ref, sems = refs[11:]
    copies = fetch(pos_ref, q_refs, kv_refs, qs, kvs, sems)
    blocks_n, span = gate_ref.shape
    blocks_all = 8 * blocks_n
    out_ref[...] = jnp.zeros_like(out_ref)
    z, y, c = pos_ref[0], pos_ref[1], pos_ref[2]
    per_owner = kvs.shape[0] // 8
    per_block = requests // blocks_n
    tok_rows = blocks_n * span
    head = qs.shape[2] // 2

    def clear(i, carry):
        code_ref[i] = 0
        return carry

    lax.fori_loop(0, code_ref.shape[0], clear, 0)

    for copy in copies[:9]:
        copy.wait()
    digits = qs[:, tok_rows : tok_rows + 16, :128].astype(F32)
    ids_vmem[...] = (digits[:, 0, :] * 32.0 + digits[:, 1, :]).astype(jnp.int32)
    to_scalars = pltpu.make_async_copy(ids_vmem, ids_ref, sems.at[len(copies)])
    to_scalars.start()
    to_scalars.wait()

    def collect(row, found):
        for j in range(per_block):
            one = ids_ref[row // blocks_n, row % blocks_n * per_block + j]
            lane = (one // per_owner) & 7
            place = ((lane & 1) ^ c) * 4 + (((lane >> 1) - y + 2) & 3)
            code_ref[found] = row * 128 + place * per_owner + one % per_owner
            found = found + (one // (8 * per_owner) == z).astype(jnp.int32)
        return found

    count = lax.fori_loop(0, blocks_all, collect, jnp.int32(0))
    code_ref[count] = 0
    count_ref[0] = count
    for copy in copies[9:]:
        copy.wait()

    def step(i, carry):
        done = []
        for u in range(2):
            at = 2 * i + u
            row, reader, block, slot = split_code(code_ref[at])
            tok = pl.ds(pl.multiple_of(block * span, span), span)
            both = qs[reader, tok]
            e, g = pair_scores(scale, both[:, :head], both[:, head:], kvs[slot])
            both = jnp.concatenate(
                [jnp.sum(e, axis=0, keepdims=True), jnp.sum(e * g, axis=0, keepdims=True)], axis=1
            )
            done.append((row, jnp.where(at < count, both, 0.0)))
        for row, both in done:
            out_ref[0, pl.ds(row, 1), :] += both
        return carry

    lax.fori_loop(0, (count + 1) // 2, step, 0)
    out_ref[0, blocks_all : blocks_all + blocks_n, 0:span] = gate_ref[...]
    for i in range(1, 8):
        out_ref[i] = out_ref[0]


def terms_kernel(scale, code_ref, count_ref, pos_ref, arrived_ref, *refs):
    q_refs, kv_refs = refs[:9], refs[9:11]
    part_refs, qout_ref, tot_ref = refs[11:15], refs[15], refs[16]
    qs, kvs, acc, qacc, gates, sems = refs[17:]
    copies = fetch(pos_ref, q_refs, kv_refs, qs, kvs, sems)
    head = qs.shape[2] // 2
    acc[...] = jnp.zeros_like(acc)
    qacc[...] = jnp.zeros_like(qacc)
    count = count_ref[0]
    blocks_all = tot_ref.shape[0]
    span = tot_ref.shape[1] // 2
    blocks_n = blocks_all // 8
    summed = jnp.sum(arrived_ref[:, :blocks_all, :], axis=0)
    lanes = lax.broadcasted_iota(jnp.int32, summed.shape, 1)
    weights = jnp.concatenate([summed[:, :span], summed[:, :span]], axis=1)
    tot_ref[...] = jnp.where(lanes < span, summed, summed / weights)
    for i in range(8):
        gates[i * blocks_n : (i + 1) * blocks_n, :] = arrived_ref[
            i, blocks_all : blocks_all + blocks_n, :
        ]
    for copy in copies:
        copy.wait()

    def step(i, carry):
        done = []
        for u in range(2):
            at = 2 * i + u
            row, reader, block, slot = split_code(code_ref[at])
            tok = pl.ds(pl.multiple_of(block * span, span), span)
            both, kv = qs[reader, tok], kvs[slot]
            q, cot = both[:, :head], both[:, head:]
            e, g = pair_scores(scale, q, cot, kv)
            tot = tot_ref[pl.ds(row, 1), :]
            gated = e * (gates[pl.ds(row, 1), :][:, :span] / tot[:, :span])
            low = gated.astype(BF)
            grad = (gated * (g - tot[:, span:])).astype(BF)
            key_term = lax.dot_general(
                grad, q, (((1,), (0,)), ((), ())), preferred_element_type=F32
            ) * scale
            value_term = lax.dot_general(
                low, cot, (((1,), (0,)), ((), ())), preferred_element_type=F32
            )
            q_term = lax.dot_general(
                grad, kv[:, : q.shape[-1]], CONTRACT_FIRST, preferred_element_type=F32
            ) * scale
            both = jnp.concatenate([key_term, value_term], axis=1).astype(BF).astype(F32)
            valid = at < count
            done.append((slot, reader, tok, jnp.where(valid, both, 0.0), jnp.where(valid, q_term, 0.0)))
        for slot, reader, tok, both, q_term in done:
            acc[slot] = (acc[slot].astype(F32) + both).astype(BF)
            qacc[reader, tok] += q_term
        return carry

    lax.fori_loop(0, (count + 1) // 2, step, 0)
    outs = []
    order = (2, 0, 3, 1)
    starts = {0: 0, 1: part_refs[0].shape[0]}
    starts[2] = starts[1] + part_refs[1].shape[0]
    starts[3] = starts[2] + part_refs[2].shape[0]
    for n in order:
        ref = part_refs[n]
        copy = pltpu.make_async_copy(acc.at[pl.ds(starts[n], ref.shape[0])], ref, sems.at[n])
        copy.start()
        outs.append(copy)
    qout_ref[...] = qacc[...].astype(BF)
    for copy in outs:
        copy.wait()


def finish_kernel(key_ref, own_ref, swapped_ref, one_ref, two_ref, out_ref):
    rows, head = key_ref.shape
    total = 0.0
    for ref in (own_ref, swapped_ref, one_ref, two_ref):
        total = total + ref[...].astype(F32).reshape(rows, 2 * head)
    key = key_ref[...].astype(F32)
    scale = lax.rsqrt(jnp.mean(key * key, axis=1, keepdims=True) + NORM_FLOOR)
    hat = total[:, :head]
    grad = scale * hat - scale * scale * scale * key * jnp.mean(key * hat, axis=1, keepdims=True)
    out_ref[:, :head] = grad.astype(BF)
    out_ref[:, head:] = total[:, head:].astype(BF)


def heads_sum(pieces, weights, columns):
    total = 0.0
    for piece, rows in zip(pieces, weights):
        term = lax.dot_general(
            piece, rows[:, columns[0] : columns[1]], CONTRACT_LAST, preferred_element_type=F32
        )
        total = total + term.astype(BF).astype(F32)
    return total.astype(BF)


def token_kernel(columns, *refs):
    far = jnp.concatenate([refs[3][...], refs[4][...]], axis=0)
    pieces = (refs[0][...], refs[1][...], refs[2][...], far)
    refs[9][...] = heads_sum(pieces, refs[5:9], columns)


def store_kernel(columns, *refs):
    weights, out_ref = refs[8:12], refs[12]
    for half in range(2):

        @pl.when(pl.program_id(0) == half)
        def _():
            pieces = tuple(ref[...] for ref in refs[4 * half : 4 * half + 4])
            out_ref[...] = heads_sum(pieces, weights, columns)


def ring4(value, axis):
    half = value.shape[0] // 2
    below = shift(value, axis, 1)
    above = shift(value, axis, -1)
    far_a = shift(below[:half], axis, 1)
    far_b = shift(above[half:], axis, -1)
    return value, above, below, far_a, far_b


def all4(value, axis):
    return value, shift(value, axis, -1), shift(value, axis, 1), shift(value, axis, 2)


def ring8(value, axis):
    half = value.shape[0] // 2
    below, above = [value], [value]
    for _ in range(3):
        below.append(shift(below[-1], axis, 1))
        above.append(shift(above[-1], axis, -1))
    far_a = shift(below[3][:half], axis, 1)
    far_b = shift(above[3][half:], axis, -1)
    return [value, above[1], above[2], above[3], far_a, below[3], below[2], below[1], far_b]


def swap(value):
    return lax.ppermute(value, "c", [(0, 1), (1, 0)])


def copy_for_each(shard, axis):
    copies = jnp.broadcast_to(shard, (lax.axis_size(axis), *shard.shape))
    return lax.all_to_all(copies, axis, split_axis=0, concat_axis=0, tiled=True)


def body(
    tokens,
    cotangent,
    mix_query,
    mix_key,
    mix_value,
    beta_pre,
    decay_pre,
    decay_rate,
    passages,
    passage_ids,
    query_weight,
    key_weight,
    value_weight,
    gate_weight,
):
    tok_rows = tokens.shape[0]
    width, head = query_weight.shape
    per_owner, rows_each = passages.shape[:2]
    blocks_n, per_block = passage_ids.shape
    span = tok_rows // blocks_n
    scale = SCORE_GAIN * head ** (-0.5)
    z, y, c, x = (lax.axis_index(a) for a in ("z", "y", "c", "x"))
    slice_w = width // 4

    pos = jnp.stack([z, y, c]).astype(jnp.int32)

    tok_pieces = all4(tokens, "x")

    flat_rows = passages.reshape(per_owner * rows_each, width)
    key_low = lax.optimization_barrier(
        jnp.dot(flat_rows, key_weight, preferred_element_type=F32).astype(BF)
    )
    value_all = jnp.dot(flat_rows, value_weight, preferred_element_type=F32).astype(BF)
    key_float = key_low.astype(F32)
    key_scale = lax.rsqrt(jnp.mean(key_float * key_float, axis=-1, keepdims=True) + NORM_FLOOR)
    key_hat = (key_float * key_scale).astype(BF)
    packed = jnp.concatenate([key_hat, value_all], axis=-1).reshape(per_owner, rows_each, 2 * head)
    kv_own = copy_for_each(packed[None], "y").reshape(4, *packed.shape)
    kv_other = swap(kv_own)

    query_acc = 0.0
    gate_acc = 0.0
    for n, piece in ((0, tok_pieces[0]), (1, tok_pieces[1]), (3, tok_pieces[2]), (2, tok_pieces[3])):
        first = ((x + n) & 3) * slice_w
        query_acc = query_acc + jnp.dot(
            piece,
            lax.dynamic_slice_in_dim(query_weight, first, slice_w, 0),
            preferred_element_type=F32,
        )
        gate_rows = lax.dynamic_slice_in_dim(gate_weight, first, slice_w, 1)
        gate_acc = gate_acc + jnp.sum(piece.astype(F32) * gate_rows.astype(F32), axis=1)
    query_low = lax.optimization_barrier(query_acc.astype(BF))
    query_float = query_low.astype(F32)
    query_scale = lax.rsqrt(
        jnp.mean(query_float * query_float, axis=-1, keepdims=True) + NORM_FLOOR
    )
    query_hat = (query_float * query_scale).astype(BF)
    gate_open = jax.nn.sigmoid(gate_acc)
    flat_ids = passage_ids.reshape(1, -1)
    digits = jnp.concatenate([flat_ids // 32, flat_ids % 32], axis=0).astype(BF)
    digits = jnp.pad(digits, ((0, 30), (0, 2 * head - digits.shape[1])))
    pieces = ring8(
        jnp.concatenate([jnp.concatenate([query_hat, cotangent], axis=1), digits], axis=0), "z"
    )

    gate_column = jnp.pad(
        jnp.broadcast_to(gate_weight.reshape(width, 1), (width, 2)), ((0, 0), (0, 126))
    )
    weights = jnp.concatenate([key_weight, value_weight, query_weight, gate_column], axis=1)
    weights, _ = lax.optimization_barrier((weights, tok_pieces[3]))
    weights = weights.reshape(4, slice_w, weights.shape[1])

    def weight_rows(step):
        rows = lax.dynamic_index_in_dim(weights, (x + step) & 3, 0, keepdims=False)
        return rows if step == 0 else shift(rows, "x", step)

    weights = [weight_rows(step) for step in (0, -1, 1, 2)]

    any_space = pl.BlockSpec(memory_space=pl.ANY)
    smem = pl.BlockSpec(memory_space=pltpu.SMEM)
    vmem = pl.BlockSpec(memory_space=pltpu.VMEM)
    stores = [
        pltpu.VMEM((8, *pieces[0].shape), BF),
        pltpu.VMEM((8 * per_owner, rows_each, 2 * head), BF),
    ]
    pieces = (*pieces, kv_own, kv_other)
    params = pltpu.CompilerParams(vmem_limit_bytes=60 * 1024 * 1024)
    message, codes, count = pl.pallas_call(
        functools.partial(sums_kernel, scale, blocks_n * per_block),
        out_shape=[
            jax.ShapeDtypeStruct((8, 9 * blocks_n, 2 * span), F32),
            jax.ShapeDtypeStruct((72,), jnp.int32),
            jax.ShapeDtypeStruct((1,), jnp.int32),
        ],
        in_specs=[smem, vmem] + [any_space] * 11,
        out_specs=[vmem, smem, smem],
        scratch_shapes=stores
        + [
            pltpu.VMEM((8, 128), jnp.int32),
            pltpu.SMEM((8, 128), jnp.int32),
            pltpu.SemaphoreType.DMA((18,)),
        ],
        compiler_params=params,
        name="sums",
    )(pos, gate_open.reshape(blocks_n, span), *pieces)
    arrived = lax.all_to_all(message, "z", split_axis=0, concat_axis=0, tiled=True)

    def part_shape(owners):
        return jax.ShapeDtypeStruct((owners * per_owner, rows_each, 2 * head), BF)

    mine_far, mine_rest, other_far, other_rest, q_parts, totals = pl.pallas_call(
        functools.partial(terms_kernel, scale),
        out_shape=[
            part_shape(1),
            part_shape(3),
            part_shape(1),
            part_shape(3),
            jax.ShapeDtypeStruct((8, tok_rows, head), BF),
            jax.ShapeDtypeStruct((8 * blocks_n, 2 * span), F32),
        ],
        in_specs=[smem, smem, smem, vmem] + [any_space] * 11,
        out_specs=[any_space] * 4 + [vmem, vmem],
        scratch_shapes=stores
        + [
            pltpu.VMEM((8 * per_owner, rows_each, 2 * head), BF),
            pltpu.VMEM((8, tok_rows, head), F32),
            pltpu.VMEM((8 * blocks_n, 2 * span), F32),
            pltpu.SemaphoreType.DMA((17,)),
        ],
        compiler_params=params,
        name="terms",
    )(codes, count, pos, arrived, *pieces)

    def plus(a, b):
        return (a.astype(F32) + b.astype(F32)).astype(BF)

    got_far = swap(other_far)
    got_rest = swap(other_rest)
    half = per_owner // 2
    got_a = shift(plus(mine_far[:half], got_far[:half]), "y", 1)
    got_b = shift(plus(mine_far[half:], got_far[half:]), "y", -1)
    near, back = 2 * per_owner, 0
    near_a, near_b, back_a, back_b = lax.optimization_barrier(
        tuple(
            plus(mine_rest[at : at + half], got_rest[at : at + half])
            for at in (near, near + half, back, back + half)
        )
    )
    early_b = shift(near_b, "y", 1)
    early_a = shift(back_a, "y", -1)
    late_a = shift(plus(near_a, got_a), "y", 1)
    late_b = shift(plus(back_b, got_b), "y", -1)

    q_back = lax.all_to_all(q_parts, "z", split_axis=0, concat_axis=0, tiled=True)
    qhat_grad = jnp.sum(q_back.astype(F32), axis=0)
    query_grad = (
        query_scale * qhat_grad
        - query_scale**3 * query_float * jnp.mean(query_float * qhat_grad, axis=-1, keepdims=True)
    ).astype(BF)
    mix_query, _ = lax.optimization_barrier((mix_query, q_parts))
    mixed_dot = mixer_dot(
        mix_query, mix_key, mix_value, cotangent, beta_pre, decay_pre, decay_rate
    ).reshape(tok_rows)
    own_totals = lax.dynamic_slice_in_dim(totals, z * blocks_n, blocks_n, 0)
    retrieved_dot = own_totals[:, span:].reshape(tok_rows)
    gate_grad = (retrieved_dot - mixed_dot) * gate_open * (1.0 - gate_open)
    high = gate_grad.astype(BF)
    rest = (gate_grad - high.astype(F32)).astype(BF)
    columns = jnp.pad(jnp.stack([high, rest], axis=1), ((0, 0), (0, 126)))
    token_pieces = ring4(jnp.concatenate([query_grad, columns], axis=1), "x")
    token_grad = pl.pallas_call(
        functools.partial(token_kernel, (2 * head, 3 * head + 128)),
        out_shape=jax.ShapeDtypeStruct((tok_rows, slice_w), BF),
        in_specs=[vmem] * 9,
        out_specs=vmem,
        compiler_params=params,
        name="token_rows",
    )(*token_pieces, *weights)

    half_rows = half * rows_each
    steps = 2
    tile = (half // steps, rows_each, 2 * head)
    tile_rows = half_rows // steps
    grads = []
    for n, one, two in ((0, early_a, late_a), (1, early_b, late_b)):
        own_part = pl.BlockSpec(tile, lambda i, n=n: (i + (2 + n) * steps, 0, 0))
        sent = pl.BlockSpec(tile, lambda i: (i, 0, 0))
        grads.append(
            pl.pallas_call(
                finish_kernel,
                grid=(steps,),
                out_shape=jax.ShapeDtypeStruct((half_rows, 2 * head), BF),
                in_specs=[
                    pl.BlockSpec((tile_rows, head), lambda i, n=n: (i + n * steps, 0)),
                    own_part,
                    own_part,
                    sent,
                    sent,
                ],
                out_specs=pl.BlockSpec((tile_rows, 2 * head), lambda i: (i, 0)),
                compiler_params=params,
            )(key_low, mine_rest, got_rest, one, two)
        )
    up_b = shift(grads[1], "x", -1)
    down_a = shift(grads[0], "x", 1)
    down_b, up_a = shift(grads[1], "x", 1), shift(grads[0], "x", -1)
    far_a, far_b = shift(down_a, "x", 1), shift(up_b, "x", -1)
    weight_b = lax.optimization_barrier(
        lax.dot_general(
            flat_rows[half_rows:], grads[1][:, :head], CONTRACT_FIRST, preferred_element_type=F32
        )
    )
    weight_term = (
        weight_b
        + lax.dot_general(
            flat_rows[:half_rows], grads[0][:, :head], CONTRACT_FIRST, preferred_element_type=F32
        )
    ).astype(BF)
    weight_term = weight_term.reshape(32, 2, width // 64, head)
    weight_other = swap(lax.dynamic_index_in_dim(weight_term, c ^ 1, 1, keepdims=False))
    weight_mine = plus(lax.dynamic_index_in_dim(weight_term, c, 1, keepdims=False), weight_other)
    weight_back = lax.all_to_all(weight_mine, ("z", "y"), split_axis=0, concat_axis=0, tiled=True)
    key_weight_grad = jnp.sum(weight_back.astype(F32), axis=0)
    passage_grad = pl.pallas_call(
        functools.partial(store_kernel, (0, 2 * head)),
        grid=(2,),
        out_shape=jax.ShapeDtypeStruct((per_owner * rows_each, slice_w), BF),
        in_specs=[pl.BlockSpec((half_rows, 2 * head), lambda i: (0, 0))] * 8
        + [pl.BlockSpec((slice_w, 2 * head), lambda i: (0, 0))] * 4,
        out_specs=pl.BlockSpec((half_rows, slice_w), lambda i: (i, 0)),
        compiler_params=params,
        name="store_rows",
    )(grads[0], up_a, down_a, far_a, grads[1], up_b, down_b, far_b, *weights).reshape(
        per_owner, rows_each, slice_w
    )
    return (token_grad, passage_grad, key_weight_grad)


def solution(mesh):
    torus = Mesh(mesh.devices.reshape(8, 4, 2, mesh.shape["tp"]), ("z", "y", "c", "x"))

    return jax.shard_map(
        body,
        mesh=torus,
        in_specs=(
            P(ST, "x"),
            P(ST, "x"),
            P(ST, "x"),
            P(ST, "x"),
            P(ST, "x"),
            P("x", ST),
            P("x", ST),
            P("x"),
            P(ST, None, None),
            P(ST, None),
            P(None, "x"),
            P(None, "x"),
            P(None, "x"),
            P("x", None),
        ),
        out_specs=(P(ST, "x"), P(ST, None, "x"), P(ST, "x")),
        check_vma=False,
    )
```

```python
import functools

import jax
import jax.numpy as jnp
from jax import lax
from jax.experimental import pallas as pl
from jax.experimental.pallas import tpu as pltpu
from jax.sharding import Mesh
from jax.sharding import PartitionSpec as P


SPAN = 64
ST = ("z", "y", "c")
NORM_FLOOR = 1.0
SCORE_GAIN = 4.0
CONTRACT_LAST = (((1,), (1,)), ((), ()))
CONTRACT_FIRST = (((0,), (0,)), ((), ()))
BF = jnp.bfloat16
F32 = jnp.float32


def shift(value, axis, step):
    n = lax.axis_size(axis)
    return lax.ppermute(value, axis, [(i, (i + step) % n) for i in range(n)])


def low_dot(a, b, dims=(((1,), (0,)), ((), ()))):
    return lax.dot_general(a.astype(BF), b.astype(BF), dims, preferred_element_type=F32)


def mixer_kernel(q_ref, k_ref, v_ref, cot_ref, rows_ref, cols_ref, out_ref):
    length, width = q_ref.shape
    heads_n = 2
    dim = width // heads_n
    blocks_n = length // SPAN
    at = lax.broadcasted_iota(jnp.int32, (SPAN, SPAN), 0)
    to = lax.broadcasted_iota(jnp.int32, (SPAN, SPAN), 1)
    eye = (at == to).astype(F32)
    pairs = [(h, n) for n in range(blocks_n) for h in range(heads_n)]
    held = {}
    for h, n in pairs:
        part = (slice(n * SPAN, (n + 1) * SPAN), slice(h * dim, (h + 1) * dim))
        q, k, v = (ref[part].astype(F32) for ref in (q_ref, k_ref, v_ref))
        q = q * lax.rsqrt(jnp.sum(q * q, axis=1, keepdims=True) + NORM_FLOOR) * dim ** (-0.5)
        k = k * lax.rsqrt(jnp.sum(k * k, axis=1, keepdims=True) + NORM_FLOOR)
        m = h * blocks_n + n
        cum_row = rows_ref[m : m + 1, :]
        cum = cols_ref[:, m : m + 1]
        strength = cols_ref[:, 2 * blocks_n + m : 2 * blocks_n + m + 1]
        last = rows_ref[m : m + 1, SPAN - 1 : SPAN]
        decay = jnp.exp(jnp.where(at >= to, cum - cum_row, -jnp.inf))
        grow = jnp.exp(cum)
        strict = jnp.where(at > to, strength * low_dot(k, k, CONTRACT_LAST) * decay, 0.0)
        attend = jnp.where(at >= to, low_dot(q, k, CONTRACT_LAST) * decay, 0.0).astype(BF)
        right = jnp.concatenate([v * strength, k * (strength * grow)], axis=1).astype(BF)
        held[h, n] = [
            strict,
            right,
            attend,
            (q * grow).astype(BF),
            (k * jnp.exp(last - cum)).astype(BF),
            jnp.exp(last),
        ]
    running = {p: eye - held[p][0] for p in pairs}
    power = {p: held[p][0] for p in pairs}
    for _ in range(SPAN.bit_length() - 2):
        for p in pairs:
            power[p] = low_dot(power[p], power[p])
        for p in pairs:
            running[p] = low_dot(running[p], eye + power[p])
    solved = {p: low_dot(running[p], held[p][1]) for p in pairs}
    state = [jnp.zeros((dim, dim), F32) for _ in range(heads_n)]
    for n in range(blocks_n):
        rows = slice(n * SPAN, (n + 1) * SPAN)
        total = 0.0
        for h in range(heads_n):
            _, _, attend, q_dec, k_dec, carry = held[h, n]
            s_low = state[h].astype(BF)
            fresh = (solved[h, n][:, :dim] - low_dot(solved[h, n][:, dim:], s_low)).astype(BF)
            out = low_dot(q_dec, s_low) + low_dot(attend, fresh)
            state[h] = state[h] * carry + low_dot(k_dec, fresh, CONTRACT_FIRST)
            cot = cot_ref[rows, h * dim : (h + 1) * dim].astype(F32)
            total = total + jnp.sum(out * cot, axis=1, keepdims=True)
        out_ref[rows, :] = total


def mixer_dot(query_raw, key_raw, value_raw, cotangent, beta_raw, decay_raw, rate_vals):
    strength = jax.nn.sigmoid(beta_raw).reshape(-1, SPAN)
    log_decay = (-rate_vals[:, None] * jax.nn.softplus(decay_raw)).reshape(-1, SPAN)
    upto = (jnp.arange(SPAN)[:, None] <= jnp.arange(SPAN)[None, :]).astype(F32)
    cumulative = jnp.dot(log_decay, upto, precision=lax.Precision.HIGHEST)
    columns = jnp.concatenate([cumulative, strength], axis=0).T
    vmem = pl.BlockSpec(memory_space=pltpu.VMEM)
    return pl.pallas_call(
        mixer_kernel,
        out_shape=jax.ShapeDtypeStruct((query_raw.shape[0], 1), F32),
        in_specs=[vmem] * 6,
        out_specs=vmem,
        name="mixer",
    )(query_raw, key_raw, value_raw, cotangent, cumulative, columns)


def fetch(pos_ref, q_refs, qs, sems):
    z = pos_ref[0]
    rows = qs.shape[1]
    copies = []

    def add(src, dst):
        copies.append(pltpu.make_async_copy(src, dst, sems.at[len(copies)]))

    for rel in range(8):
        slot = (z + rel) & 7
        if rel == 4:
            add(q_refs[4], qs.at[slot, pl.ds(0, rows // 2)])
            add(q_refs[8], qs.at[slot, pl.ds(rows // 2, rows // 2)])
        else:
            add(q_refs[rel], qs.at[slot])
    for copy in copies:
        copy.start()
    return copies


def fetch_passages(total, code_ref, y, kv_refs, kvs, kv_sems):
    per = kv_refs[0].shape[1]

    def start(i, carry):
        slot = code_ref[i] & 127
        place = slot // per
        at = (y + place + 2) & 3
        for other in range(2):

            @pl.when(place // 4 == other)
            def _():
                pltpu.make_async_copy(
                    kv_refs[other].at[at, slot % per], kvs.at[i], kv_sems.at[i]
                ).start()

        return carry

    lax.fori_loop(0, total, start, 0)


def wait_passage(i, kv_refs, kvs, kv_sems):
    pltpu.make_async_copy(kv_refs[0].at[0, 0], kvs.at[i], kv_sems.at[i]).wait()


def split_code(code):
    row = code >> 7
    return row, row // 6, row % 6, code & 127


def pair_scores(scale, q, cot, kv):
    head = q.shape[-1]
    scores = lax.dot_general(kv[:, :head], q, CONTRACT_LAST, preferred_element_type=F32) * scale
    grads = lax.dot_general(kv[:, head:], cot, CONTRACT_LAST, preferred_element_type=F32)
    return jnp.exp(scores), grads


def sums_kernel(scale, requests, pos_ref, gate_ref, *refs):
    q_refs, kv_refs = refs[:9], refs[9:11]
    out_ref, code_ref, count_ref, qs, kvs, ids_vmem, ids_ref, sems, kv_sems = refs[11:]
    copies = fetch(pos_ref, q_refs, qs, sems)
    blocks_n, span = gate_ref.shape
    blocks_all = 8 * blocks_n
    out_ref[...] = jnp.zeros_like(out_ref)
    z, y, c = pos_ref[0], pos_ref[1], pos_ref[2]
    per_owner = kv_refs[0].shape[1]
    per_block = requests // blocks_n
    tok_rows = blocks_n * span
    head = qs.shape[2] // 2

    def clear(i, carry):
        code_ref[i] = 0
        return carry

    lax.fori_loop(0, code_ref.shape[0], clear, 0)

    for copy in copies:
        copy.wait()
    digits = qs[:, tok_rows : tok_rows + 16, :128].astype(F32)
    ids_vmem[...] = (digits[:, 0, :] * 32.0 + digits[:, 1, :]).astype(jnp.int32)
    to_scalars = pltpu.make_async_copy(ids_vmem, ids_ref, sems.at[len(copies)])
    to_scalars.start()
    to_scalars.wait()

    def collect(row, found):
        for j in range(per_block):
            one = ids_ref[row // blocks_n, row % blocks_n * per_block + j]
            lane = (one // per_owner) & 7
            place = ((lane & 1) ^ c) * 4 + (((lane >> 1) - y + 2) & 3)
            code_ref[found] = row * 128 + place * per_owner + one % per_owner
            found = found + (one // (8 * per_owner) == z).astype(jnp.int32)
        return found

    count = lax.fori_loop(0, blocks_all, collect, jnp.int32(0))
    code_ref[count] = 0
    count_ref[0] = count
    steps = (count + 1) // 2
    fetch_passages(2 * steps, code_ref, y, kv_refs, kvs, kv_sems)

    def step(i, carry):
        done = []
        for u in range(2):
            wait_passage(2 * i + u, kv_refs, kvs, kv_sems)
        for u in range(2):
            at = 2 * i + u
            row, reader, block, _ = split_code(code_ref[at])
            tok = pl.ds(pl.multiple_of(block * span, span), span)
            both = qs[reader, tok]
            e, g = pair_scores(scale, both[:, :head], both[:, head:], kvs[at])
            both = jnp.concatenate(
                [jnp.sum(e, axis=0, keepdims=True), jnp.sum(e * g, axis=0, keepdims=True)], axis=1
            )
            done.append((row, jnp.where(at < count, both, 0.0)))
        for row, both in done:
            out_ref[0, pl.ds(row, 1), :] += both
        return carry

    lax.fori_loop(0, steps, step, 0)
    out_ref[0, blocks_all : blocks_all + blocks_n, 0:span] = gate_ref[...]
    for i in range(1, 8):
        out_ref[i] = out_ref[0]


def terms_kernel(scale, code_ref, count_ref, pos_ref, arrived_ref, *refs):
    q_refs, kv_refs = refs[:9], refs[9:11]
    part_refs, qout_ref, tot_ref = refs[11:15], refs[15], refs[16]
    qs, kvs, acc, qacc, gates, sems, kv_sems = refs[17:]
    copies = fetch(pos_ref, q_refs, qs, sems)
    steps = (count_ref[0] + 1) // 2
    fetch_passages(2 * steps, code_ref, pos_ref[1], kv_refs, kvs, kv_sems)
    head = qs.shape[2] // 2
    acc[...] = jnp.zeros_like(acc)
    qacc[...] = jnp.zeros_like(qacc)
    count = count_ref[0]
    blocks_all = tot_ref.shape[0]
    span = tot_ref.shape[1] // 2
    blocks_n = blocks_all // 8
    summed = jnp.sum(arrived_ref[:, :blocks_all, :], axis=0)
    lanes = lax.broadcasted_iota(jnp.int32, summed.shape, 1)
    weights = jnp.concatenate([summed[:, :span], summed[:, :span]], axis=1)
    tot_ref[...] = jnp.where(lanes < span, summed, summed / weights)
    for i in range(8):
        gates[i * blocks_n : (i + 1) * blocks_n, :] = arrived_ref[
            i, blocks_all : blocks_all + blocks_n, :
        ]
    for copy in copies:
        copy.wait()

    def step(i, carry):
        done = []
        for u in range(2):
            wait_passage(2 * i + u, kv_refs, kvs, kv_sems)
        for u in range(2):
            at = 2 * i + u
            row, reader, block, slot = split_code(code_ref[at])
            tok = pl.ds(pl.multiple_of(block * span, span), span)
            both, kv = qs[reader, tok], kvs[at]
            q, cot = both[:, :head], both[:, head:]
            e, g = pair_scores(scale, q, cot, kv)
            tot = tot_ref[pl.ds(row, 1), :]
            gated = e * (gates[pl.ds(row, 1), :][:, :span] / tot[:, :span])
            low = gated.astype(BF)
            grad = (gated * (g - tot[:, span:])).astype(BF)
            key_term = lax.dot_general(
                grad, q, (((1,), (0,)), ((), ())), preferred_element_type=F32
            ) * scale
            value_term = lax.dot_general(
                low, cot, (((1,), (0,)), ((), ())), preferred_element_type=F32
            )
            q_term = lax.dot_general(
                grad, kv[:, : q.shape[-1]], CONTRACT_FIRST, preferred_element_type=F32
            ) * scale
            both = jnp.concatenate([key_term, value_term], axis=1).astype(BF).astype(F32)
            valid = at < count
            done.append((slot, reader, tok, jnp.where(valid, both, 0.0), jnp.where(valid, q_term, 0.0)))
        for slot, reader, tok, both, q_term in done:
            acc[slot] = (acc[slot].astype(F32) + both).astype(BF)
            qacc[reader, tok] += q_term
        return carry

    lax.fori_loop(0, steps, step, 0)
    outs = []
    order = (2, 0, 3, 1)
    starts = {0: 0, 1: part_refs[0].shape[0]}
    starts[2] = starts[1] + part_refs[1].shape[0]
    starts[3] = starts[2] + part_refs[2].shape[0]
    for n in order:
        ref = part_refs[n]
        copy = pltpu.make_async_copy(acc.at[pl.ds(starts[n], ref.shape[0])], ref, sems.at[n])
        copy.start()
        outs.append(copy)
    qout_ref[...] = qacc[...].astype(BF)
    for copy in outs:
        copy.wait()


def finish_kernel(key_ref, own_ref, swapped_ref, one_ref, two_ref, out_ref):
    rows, head = key_ref.shape
    total = 0.0
    for ref in (own_ref, swapped_ref, one_ref, two_ref):
        total = total + ref[...].astype(F32).reshape(rows, 2 * head)
    key = key_ref[...].astype(F32)
    scale = lax.rsqrt(jnp.mean(key * key, axis=1, keepdims=True) + NORM_FLOOR)
    hat = total[:, :head]
    grad = scale * hat - scale * scale * scale * key * jnp.mean(key * hat, axis=1, keepdims=True)
    out_ref[:, :head] = grad.astype(BF)
    out_ref[:, head:] = total[:, head:].astype(BF)


def heads_sum(pieces, weights, columns):
    total = 0.0
    for piece, rows in zip(pieces, weights):
        term = lax.dot_general(
            piece, rows[:, columns[0] : columns[1]], CONTRACT_LAST, preferred_element_type=F32
        )
        total = total + term.astype(BF).astype(F32)
    return total.astype(BF)


def token_kernel(columns, *refs):
    far = jnp.concatenate([refs[3][...], refs[4][...]], axis=0)
    pieces = (refs[0][...], refs[1][...], refs[2][...], far)
    refs[9][...] = heads_sum(pieces, refs[5:9], columns)


def store_kernel(columns, *refs):
    weights, out_ref = refs[8:12], refs[12]
    for half in range(2):

        @pl.when(pl.program_id(0) == half)
        def _():
            pieces = tuple(ref[...] for ref in refs[4 * half : 4 * half + 4])
            out_ref[...] = heads_sum(pieces, weights, columns)


def ring4(value, axis):
    half = value.shape[0] // 2
    below = shift(value, axis, 1)
    above = shift(value, axis, -1)
    far_a = shift(below[:half], axis, 1)
    far_b = shift(above[half:], axis, -1)
    return value, above, below, far_a, far_b


def all4(value, axis):
    return value, shift(value, axis, -1), shift(value, axis, 1), shift(value, axis, 2)


def ring8(value, axis):
    half = value.shape[0] // 2
    below, above = [value], [value]
    for _ in range(3):
        below.append(shift(below[-1], axis, 1))
        above.append(shift(above[-1], axis, -1))
    far_a = shift(below[3][:half], axis, 1)
    far_b = shift(above[3][half:], axis, -1)
    return [value, above[1], above[2], above[3], far_a, below[3], below[2], below[1], far_b]


def swap(value):
    return lax.ppermute(value, "c", [(0, 1), (1, 0)])


def copy_for_each(shard, axis):
    copies = jnp.broadcast_to(shard, (lax.axis_size(axis), *shard.shape))
    return lax.all_to_all(copies, axis, split_axis=0, concat_axis=0, tiled=True)


def body(
    tokens,
    cotangent,
    mix_query,
    mix_key,
    mix_value,
    beta_pre,
    decay_pre,
    decay_rate,
    passages,
    passage_ids,
    query_weight,
    key_weight,
    value_weight,
    gate_weight,
):
    tok_rows = tokens.shape[0]
    width, head = query_weight.shape
    per_owner, rows_each = passages.shape[:2]
    blocks_n, per_block = passage_ids.shape
    span = tok_rows // blocks_n
    scale = SCORE_GAIN * head ** (-0.5)
    z, y, c, x = (lax.axis_index(a) for a in ("z", "y", "c", "x"))
    slice_w = width // 4

    pos = jnp.stack([z, y, c]).astype(jnp.int32)

    tok_pieces = all4(tokens, "x")

    flat_rows = passages.reshape(per_owner * rows_each, width)
    key_low = lax.optimization_barrier(
        jnp.dot(flat_rows, key_weight, preferred_element_type=F32).astype(BF)
    )
    value_all = jnp.dot(flat_rows, value_weight, preferred_element_type=F32).astype(BF)
    key_float = key_low.astype(F32)
    key_scale = lax.rsqrt(jnp.mean(key_float * key_float, axis=-1, keepdims=True) + NORM_FLOOR)
    key_hat = (key_float * key_scale).astype(BF)
    packed = jnp.concatenate([key_hat, value_all], axis=-1).reshape(per_owner, rows_each, 2 * head)
    kv_own = copy_for_each(packed[None], "y").reshape(4, *packed.shape)
    kv_other = swap(kv_own)

    query_acc = 0.0
    gate_acc = 0.0
    for n, piece in ((0, tok_pieces[0]), (1, tok_pieces[1]), (3, tok_pieces[2]), (2, tok_pieces[3])):
        first = ((x + n) & 3) * slice_w
        query_acc = query_acc + jnp.dot(
            piece,
            lax.dynamic_slice_in_dim(query_weight, first, slice_w, 0),
            preferred_element_type=F32,
        )
        gate_rows = lax.dynamic_slice_in_dim(gate_weight, first, slice_w, 1)
        gate_acc = gate_acc + jnp.sum(piece.astype(F32) * gate_rows.astype(F32), axis=1)
    query_low = lax.optimization_barrier(query_acc.astype(BF))
    query_float = query_low.astype(F32)
    query_scale = lax.rsqrt(
        jnp.mean(query_float * query_float, axis=-1, keepdims=True) + NORM_FLOOR
    )
    query_hat = (query_float * query_scale).astype(BF)
    gate_open = jax.nn.sigmoid(gate_acc)
    flat_ids = passage_ids.reshape(1, -1)
    digits = jnp.concatenate([flat_ids // 32, flat_ids % 32], axis=0).astype(BF)
    digits = jnp.pad(digits, ((0, 30), (0, 2 * head - digits.shape[1])))
    pieces = ring8(
        jnp.concatenate([jnp.concatenate([query_hat, cotangent], axis=1), digits], axis=0), "z"
    )

    gate_column = jnp.pad(
        jnp.broadcast_to(gate_weight.reshape(width, 1), (width, 2)), ((0, 0), (0, 126))
    )
    weights = jnp.concatenate([key_weight, value_weight, query_weight, gate_column], axis=1)
    weights, _ = lax.optimization_barrier((weights, tok_pieces[3]))
    weights = weights.reshape(4, slice_w, weights.shape[1])

    def weight_rows(step):
        rows = lax.dynamic_index_in_dim(weights, (x + step) & 3, 0, keepdims=False)
        return rows if step == 0 else shift(rows, "x", step)

    weights = [weight_rows(step) for step in (0, -1, 1, 2)]

    any_space = pl.BlockSpec(memory_space=pl.ANY)
    smem = pl.BlockSpec(memory_space=pltpu.SMEM)
    vmem = pl.BlockSpec(memory_space=pltpu.VMEM)
    stores = [
        pltpu.VMEM((8, *pieces[0].shape), BF),
        pltpu.VMEM((64, rows_each, 2 * head), BF),
    ]
    pieces = (*pieces, kv_own, kv_other)
    params = pltpu.CompilerParams(vmem_limit_bytes=60 * 1024 * 1024)
    message, codes, count = pl.pallas_call(
        functools.partial(sums_kernel, scale, blocks_n * per_block),
        out_shape=[
            jax.ShapeDtypeStruct((8, 9 * blocks_n, 2 * span), F32),
            jax.ShapeDtypeStruct((72,), jnp.int32),
            jax.ShapeDtypeStruct((1,), jnp.int32),
        ],
        in_specs=[smem, vmem] + [any_space] * 11,
        out_specs=[vmem, smem, smem],
        scratch_shapes=stores
        + [
            pltpu.VMEM((8, 128), jnp.int32),
            pltpu.SMEM((8, 128), jnp.int32),
            pltpu.SemaphoreType.DMA((10,)),
            pltpu.SemaphoreType.DMA((64,)),
        ],
        compiler_params=params,
        name="sums",
    )(pos, gate_open.reshape(blocks_n, span), *pieces)
    arrived = lax.all_to_all(message, "z", split_axis=0, concat_axis=0, tiled=True)

    def part_shape(owners):
        return jax.ShapeDtypeStruct((owners * per_owner, rows_each, 2 * head), BF)

    mine_far, mine_rest, other_far, other_rest, q_parts, totals = pl.pallas_call(
        functools.partial(terms_kernel, scale),
        out_shape=[
            part_shape(1),
            part_shape(3),
            part_shape(1),
            part_shape(3),
            jax.ShapeDtypeStruct((8, tok_rows, head), BF),
            jax.ShapeDtypeStruct((8 * blocks_n, 2 * span), F32),
        ],
        in_specs=[smem, smem, smem, vmem] + [any_space] * 11,
        out_specs=[any_space] * 4 + [vmem, vmem],
        scratch_shapes=stores
        + [
            pltpu.VMEM((8 * per_owner, rows_each, 2 * head), BF),
            pltpu.VMEM((8, tok_rows, head), F32),
            pltpu.VMEM((8 * blocks_n, 2 * span), F32),
            pltpu.SemaphoreType.DMA((9,)),
            pltpu.SemaphoreType.DMA((64,)),
        ],
        compiler_params=params,
        name="terms",
    )(codes, count, pos, arrived, *pieces)

    def plus(a, b):
        return (a.astype(F32) + b.astype(F32)).astype(BF)

    got_far = swap(other_far)
    got_rest = swap(other_rest)
    half = per_owner // 2
    got_a = shift(plus(mine_far[:half], got_far[:half]), "y", 1)
    got_b = shift(plus(mine_far[half:], got_far[half:]), "y", -1)
    near, back = 2 * per_owner, 0
    near_a, near_b, back_a, back_b = lax.optimization_barrier(
        tuple(
            plus(mine_rest[at : at + half], got_rest[at : at + half])
            for at in (near, near + half, back, back + half)
        )
    )
    early_b = shift(near_b, "y", 1)
    early_a = shift(back_a, "y", -1)
    late_a = shift(plus(near_a, got_a), "y", 1)
    late_b = shift(plus(back_b, got_b), "y", -1)

    q_back = lax.all_to_all(q_parts, "z", split_axis=0, concat_axis=0, tiled=True)
    qhat_grad = jnp.sum(q_back.astype(F32), axis=0)
    query_grad = (
        query_scale * qhat_grad
        - query_scale**3 * query_float * jnp.mean(query_float * qhat_grad, axis=-1, keepdims=True)
    ).astype(BF)
    mix_query, _ = lax.optimization_barrier((mix_query, q_parts))
    mixed_dot = mixer_dot(
        mix_query, mix_key, mix_value, cotangent, beta_pre, decay_pre, decay_rate
    ).reshape(tok_rows)
    own_totals = lax.dynamic_slice_in_dim(totals, z * blocks_n, blocks_n, 0)
    retrieved_dot = own_totals[:, span:].reshape(tok_rows)
    gate_grad = (retrieved_dot - mixed_dot) * gate_open * (1.0 - gate_open)
    high = gate_grad.astype(BF)
    rest = (gate_grad - high.astype(F32)).astype(BF)
    columns = jnp.pad(jnp.stack([high, rest], axis=1), ((0, 0), (0, 126)))
    token_pieces = ring4(jnp.concatenate([query_grad, columns], axis=1), "x")
    token_grad = pl.pallas_call(
        functools.partial(token_kernel, (2 * head, 3 * head + 128)),
        out_shape=jax.ShapeDtypeStruct((tok_rows, slice_w), BF),
        in_specs=[vmem] * 9,
        out_specs=vmem,
        compiler_params=params,
        name="token_rows",
    )(*token_pieces, *weights)

    half_rows = half * rows_each
    steps = 2
    tile = (half // steps, rows_each, 2 * head)
    tile_rows = half_rows // steps
    grads = []
    for n, one, two in ((0, early_a, late_a), (1, early_b, late_b)):
        own_part = pl.BlockSpec(tile, lambda i, n=n: (i + (2 + n) * steps, 0, 0))
        sent = pl.BlockSpec(tile, lambda i: (i, 0, 0))
        grads.append(
            pl.pallas_call(
                finish_kernel,
                grid=(steps,),
                out_shape=jax.ShapeDtypeStruct((half_rows, 2 * head), BF),
                in_specs=[
                    pl.BlockSpec((tile_rows, head), lambda i, n=n: (i + n * steps, 0)),
                    own_part,
                    own_part,
                    sent,
                    sent,
                ],
                out_specs=pl.BlockSpec((tile_rows, 2 * head), lambda i: (i, 0)),
                compiler_params=params,
            )(key_low, mine_rest, got_rest, one, two)
        )
    up_b = shift(grads[1], "x", -1)
    down_a = shift(grads[0], "x", 1)
    down_b, up_a = shift(grads[1], "x", 1), shift(grads[0], "x", -1)
    far_a, far_b = shift(down_a, "x", 1), shift(up_b, "x", -1)
    weight_b = lax.optimization_barrier(
        lax.dot_general(
            flat_rows[half_rows:], grads[1][:, :head], CONTRACT_FIRST, preferred_element_type=F32
        )
    )
    weight_term = (
        weight_b
        + lax.dot_general(
            flat_rows[:half_rows], grads[0][:, :head], CONTRACT_FIRST, preferred_element_type=F32
        )
    ).astype(BF)
    weight_term = weight_term.reshape(32, 2, width // 64, head)
    weight_other = swap(lax.dynamic_index_in_dim(weight_term, c ^ 1, 1, keepdims=False))
    weight_mine = plus(lax.dynamic_index_in_dim(weight_term, c, 1, keepdims=False), weight_other)
    weight_back = lax.all_to_all(weight_mine, ("z", "y"), split_axis=0, concat_axis=0, tiled=True)
    key_weight_grad = jnp.sum(weight_back.astype(F32), axis=0)
    passage_grad = pl.pallas_call(
        functools.partial(store_kernel, (0, 2 * head)),
        grid=(2,),
        out_shape=jax.ShapeDtypeStruct((per_owner * rows_each, slice_w), BF),
        in_specs=[pl.BlockSpec((half_rows, 2 * head), lambda i: (0, 0))] * 8
        + [pl.BlockSpec((slice_w, 2 * head), lambda i: (0, 0))] * 4,
        out_specs=pl.BlockSpec((half_rows, slice_w), lambda i: (i, 0)),
        compiler_params=params,
        name="store_rows",
    )(grads[0], up_a, down_a, far_a, grads[1], up_b, down_b, far_b, *weights).reshape(
        per_owner, rows_each, slice_w
    )
    return (token_grad, passage_grad, key_weight_grad)


def solution(mesh):
    torus = Mesh(mesh.devices.reshape(8, 4, 2, mesh.shape["tp"]), ("z", "y", "c", "x"))

    return jax.shard_map(
        body,
        mesh=torus,
        in_specs=(
            P(ST, "x"),
            P(ST, "x"),
            P(ST, "x"),
            P(ST, "x"),
            P(ST, "x"),
            P("x", ST),
            P("x", ST),
            P("x"),
            P(ST, None, None),
            P(ST, None),
            P(None, "x"),
            P(None, "x"),
            P(None, "x"),
            P("x", None),
        ),
        out_specs=(P(ST, "x"), P(ST, None, "x"), P(ST, "x")),
        check_vma=False,
    )
```

```python
import functools

import jax
import jax.numpy as jnp
from jax import lax
from jax.experimental import pallas as pl
from jax.experimental.pallas import tpu as pltpu
from jax.sharding import Mesh
from jax.sharding import PartitionSpec as P


SPAN = 64
ST = ("z", "y", "c")
NORM_FLOOR = 1.0
SCORE_GAIN = 4.0
CONTRACT_LAST = (((1,), (1,)), ((), ()))
CONTRACT_FIRST = (((0,), (0,)), ((), ()))
BF = jnp.bfloat16
F32 = jnp.float32


def shift(value, axis, step):
    n = lax.axis_size(axis)
    return lax.ppermute(value, axis, [(i, (i + step) % n) for i in range(n)])


def low_dot(a, b, dims=(((1,), (0,)), ((), ()))):
    return lax.dot_general(a.astype(BF), b.astype(BF), dims, preferred_element_type=F32)


def mixer_kernel(q_ref, k_ref, v_ref, cot_ref, rows_ref, cols_ref, out_ref):
    length, width = q_ref.shape
    heads_n = 2
    dim = width // heads_n
    blocks_n = length // SPAN
    at = lax.broadcasted_iota(jnp.int32, (SPAN, SPAN), 0)
    to = lax.broadcasted_iota(jnp.int32, (SPAN, SPAN), 1)
    eye = (at == to).astype(F32)
    pairs = [(h, n) for n in range(blocks_n) for h in range(heads_n)]
    held = {}
    for h, n in pairs:
        part = (slice(n * SPAN, (n + 1) * SPAN), slice(h * dim, (h + 1) * dim))
        q, k, v = (ref[part].astype(F32) for ref in (q_ref, k_ref, v_ref))
        q = q * lax.rsqrt(jnp.sum(q * q, axis=1, keepdims=True) + NORM_FLOOR) * dim ** (-0.5)
        k = k * lax.rsqrt(jnp.sum(k * k, axis=1, keepdims=True) + NORM_FLOOR)
        m = h * blocks_n + n
        cum_row = rows_ref[m : m + 1, :]
        cum = cols_ref[:, m : m + 1]
        strength = cols_ref[:, 2 * blocks_n + m : 2 * blocks_n + m + 1]
        last = rows_ref[m : m + 1, SPAN - 1 : SPAN]
        decay = jnp.exp(jnp.where(at >= to, cum - cum_row, -jnp.inf))
        grow = jnp.exp(cum)
        strict = jnp.where(at > to, strength * low_dot(k, k, CONTRACT_LAST) * decay, 0.0)
        attend = jnp.where(at >= to, low_dot(q, k, CONTRACT_LAST) * decay, 0.0).astype(BF)
        right = jnp.concatenate([v * strength, k * (strength * grow)], axis=1).astype(BF)
        held[h, n] = [
            strict,
            right,
            attend,
            (q * grow).astype(BF),
            (k * jnp.exp(last - cum)).astype(BF),
            jnp.exp(last),
        ]
    running = {p: eye - held[p][0] for p in pairs}
    power = {p: held[p][0] for p in pairs}
    for _ in range(SPAN.bit_length() - 2):
        for p in pairs:
            power[p] = low_dot(power[p], power[p])
        for p in pairs:
            running[p] = low_dot(running[p], eye + power[p])
    solved = {p: low_dot(running[p], held[p][1]) for p in pairs}
    state = [jnp.zeros((dim, dim), F32) for _ in range(heads_n)]
    for n in range(blocks_n):
        rows = slice(n * SPAN, (n + 1) * SPAN)
        total = 0.0
        for h in range(heads_n):
            _, _, attend, q_dec, k_dec, carry = held[h, n]
            s_low = state[h].astype(BF)
            fresh = (solved[h, n][:, :dim] - low_dot(solved[h, n][:, dim:], s_low)).astype(BF)
            out = low_dot(q_dec, s_low) + low_dot(attend, fresh)
            state[h] = state[h] * carry + low_dot(k_dec, fresh, CONTRACT_FIRST)
            cot = cot_ref[rows, h * dim : (h + 1) * dim].astype(F32)
            total = total + jnp.sum(out * cot, axis=1, keepdims=True)
        out_ref[rows, :] = total


def mixer_dot(query_raw, key_raw, value_raw, cotangent, beta_raw, decay_raw, rate_vals):
    strength = jax.nn.sigmoid(beta_raw).reshape(-1, SPAN)
    log_decay = (-rate_vals[:, None] * jax.nn.softplus(decay_raw)).reshape(-1, SPAN)
    upto = (jnp.arange(SPAN)[:, None] <= jnp.arange(SPAN)[None, :]).astype(F32)
    cumulative = jnp.dot(log_decay, upto, precision=lax.Precision.HIGHEST)
    columns = jnp.concatenate([cumulative, strength], axis=0).T
    vmem = pl.BlockSpec(memory_space=pltpu.VMEM)
    return pl.pallas_call(
        mixer_kernel,
        out_shape=jax.ShapeDtypeStruct((query_raw.shape[0], 1), F32),
        in_specs=[vmem] * 6,
        out_specs=vmem,
        name="mixer",
    )(query_raw, key_raw, value_raw, cotangent, cumulative, columns)


def fetch(pos_ref, q_refs, qs, sems):
    z = pos_ref[0]
    rows = qs.shape[1]
    copies = []

    def add(src, dst):
        copies.append(pltpu.make_async_copy(src, dst, sems.at[len(copies)]))

    for rel in range(8):
        slot = (z + rel) & 7
        if rel == 4:
            add(q_refs[4], qs.at[slot, pl.ds(0, rows // 2)])
            add(q_refs[8], qs.at[slot, pl.ds(rows // 2, rows // 2)])
        else:
            add(q_refs[rel], qs.at[slot])
    for copy in copies:
        copy.start()
    return copies


def fetch_passages(total, code_ref, y, kv_refs, kvs, kv_sems):
    per = kv_refs[0].shape[1]

    def start(i, carry):
        slot = code_ref[i] & 127
        place = slot // per
        at = (y + place + 2) & 3
        for other in range(2):

            @pl.when(place // 4 == other)
            def _():
                pltpu.make_async_copy(
                    kv_refs[other].at[at, slot % per], kvs.at[i], kv_sems.at[i]
                ).start()

        return carry

    lax.fori_loop(0, total, start, 0)


def wait_passage(i, kv_refs, kvs, kv_sems):
    pltpu.make_async_copy(kv_refs[0].at[0, 0], kvs.at[i], kv_sems.at[i]).wait()


def split_code(code, blocks_n):
    reader, block = code >> 10, (code >> 7) & 7
    return reader * blocks_n + block, reader, block, code & 127


def pair_scores(scale, q, cot, kv):
    head = q.shape[-1]
    scores = lax.dot_general(kv[:, :head], q, CONTRACT_LAST, preferred_element_type=F32) * scale
    grads = lax.dot_general(kv[:, head:], cot, CONTRACT_LAST, preferred_element_type=F32)
    return jnp.exp(scores), grads


def sums_kernel(scale, requests, pos_ref, gate_ref, *refs):
    q_refs, kv_refs = refs[:9], refs[9:11]
    out_ref, code_ref, count_ref, qs, kvs, ids_vmem, ids_ref, sems, kv_sems = refs[11:]
    copies = fetch(pos_ref, q_refs, qs, sems)
    blocks_n, span = gate_ref.shape
    blocks_all = 8 * blocks_n
    out_ref[...] = jnp.zeros_like(out_ref)
    z, y, c = pos_ref[0], pos_ref[1], pos_ref[2]
    per_owner = kv_refs[0].shape[1]
    per_block = requests // blocks_n
    tok_rows = blocks_n * span
    head = qs.shape[2] // 2

    for copy in copies:
        copy.wait()
    digits = qs[:, tok_rows : tok_rows + 16, :128].astype(F32)
    ids_vmem[...] = (digits[:, 0, :] * 32.0 + digits[:, 1, :]).astype(jnp.int32)
    to_scalars = pltpu.make_async_copy(ids_vmem, ids_ref, sems.at[len(copies)])
    to_scalars.start()
    to_scalars.wait()

    bits = per_owner.bit_length() - 1

    def collect(reader, found):
        for n in range(requests):
            one = ids_ref[reader, n]
            lane = (one >> bits) & 7
            place = ((lane & 1) ^ c) * 4 + (((lane >> 1) - y + 2) & 3)
            block = n // per_block
            code_ref[found] = (reader * 8 + block) * 128 + place * per_owner + (one & (per_owner - 1))
            found = found + ((one >> (bits + 3)) == z).astype(jnp.int32)
        return found

    count = lax.fori_loop(0, 8, collect, jnp.int32(0))
    code_ref[count] = 0
    count_ref[0] = count
    steps = (count + 1) // 2
    fetch_passages(2 * steps, code_ref, y, kv_refs, kvs, kv_sems)

    def step(i, carry):
        done = []
        for u in range(2):
            wait_passage(2 * i + u, kv_refs, kvs, kv_sems)
        for u in range(2):
            at = 2 * i + u
            row, reader, block, _ = split_code(code_ref[at], blocks_n)
            tok = pl.ds(pl.multiple_of(block * span, span), span)
            both = qs[reader, tok]
            e, g = pair_scores(scale, both[:, :head], both[:, head:], kvs[at])
            both = jnp.concatenate(
                [jnp.sum(e, axis=0, keepdims=True), jnp.sum(e * g, axis=0, keepdims=True)], axis=1
            )
            done.append((row, jnp.where(at < count, both, 0.0)))
        for row, both in done:
            out_ref[0, pl.ds(row, 1), :] += both
        return carry

    lax.fori_loop(0, steps, step, 0)
    out_ref[0, blocks_all : blocks_all + blocks_n, 0:span] = gate_ref[...]
    for i in range(1, 8):
        out_ref[i] = out_ref[0]


def terms_kernel(scale, code_ref, count_ref, pos_ref, arrived_ref, *refs):
    q_refs, kv_refs = refs[:9], refs[9:11]
    part_refs, qout_ref, tot_ref = refs[11:15], refs[15], refs[16]
    qs, kvs, acc, qacc, gates, sems, kv_sems = refs[17:]
    copies = fetch(pos_ref, q_refs, qs, sems)
    steps = (count_ref[0] + 1) // 2
    fetch_passages(2 * steps, code_ref, pos_ref[1], kv_refs, kvs, kv_sems)
    head = qs.shape[2] // 2
    acc[...] = jnp.zeros_like(acc)
    qacc[...] = jnp.zeros_like(qacc)
    count = count_ref[0]
    blocks_all = tot_ref.shape[0]
    span = tot_ref.shape[1] // 2
    blocks_n = blocks_all // 8
    summed = jnp.sum(arrived_ref[:, :blocks_all, :], axis=0)
    lanes = lax.broadcasted_iota(jnp.int32, summed.shape, 1)
    weights = jnp.concatenate([summed[:, :span], summed[:, :span]], axis=1)
    tot_ref[...] = jnp.where(lanes < span, summed, summed / weights)
    for i in range(8):
        gates[i * blocks_n : (i + 1) * blocks_n, :] = arrived_ref[
            i, blocks_all : blocks_all + blocks_n, :
        ]
    for copy in copies:
        copy.wait()

    def step(i, carry):
        done = []
        for u in range(2):
            wait_passage(2 * i + u, kv_refs, kvs, kv_sems)
        for u in range(2):
            at = 2 * i + u
            row, reader, block, slot = split_code(code_ref[at], blocks_n)
            tok = pl.ds(pl.multiple_of(block * span, span), span)
            both, kv = qs[reader, tok], kvs[at]
            q, cot = both[:, :head], both[:, head:]
            e, g = pair_scores(scale, q, cot, kv)
            tot = tot_ref[pl.ds(row, 1), :]
            gated = e * (gates[pl.ds(row, 1), :][:, :span] / tot[:, :span])
            low = gated.astype(BF)
            grad = (gated * (g - tot[:, span:])).astype(BF)
            key_term = lax.dot_general(
                grad, q, (((1,), (0,)), ((), ())), preferred_element_type=F32
            ) * scale
            value_term = lax.dot_general(
                low, cot, (((1,), (0,)), ((), ())), preferred_element_type=F32
            )
            q_term = lax.dot_general(
                grad, kv[:, : q.shape[-1]], CONTRACT_FIRST, preferred_element_type=F32
            ) * scale
            both = jnp.concatenate([key_term, value_term], axis=1).astype(BF).astype(F32)
            valid = at < count
            done.append((slot, reader, tok, jnp.where(valid, both, 0.0), jnp.where(valid, q_term, 0.0)))
        for slot, reader, tok, both, q_term in done:
            acc[slot] = (acc[slot].astype(F32) + both).astype(BF)
            qacc[reader, tok] += q_term
        return carry

    lax.fori_loop(0, steps, step, 0)
    outs = []
    order = (2, 0, 3, 1)
    starts = {0: 0, 1: part_refs[0].shape[0]}
    starts[2] = starts[1] + part_refs[1].shape[0]
    starts[3] = starts[2] + part_refs[2].shape[0]
    for n in order:
        ref = part_refs[n]
        copy = pltpu.make_async_copy(acc.at[pl.ds(starts[n], ref.shape[0])], ref, sems.at[n])
        copy.start()
        outs.append(copy)
    qout_ref[...] = qacc[...].astype(BF)
    for copy in outs:
        copy.wait()


def finish_kernel(key_ref, own_ref, swapped_ref, one_ref, two_ref, out_ref):
    rows, head = key_ref.shape
    total = 0.0
    for ref in (own_ref, swapped_ref, one_ref, two_ref):
        total = total + ref[...].astype(F32).reshape(rows, 2 * head)
    key = key_ref[...].astype(F32)
    scale = lax.rsqrt(jnp.mean(key * key, axis=1, keepdims=True) + NORM_FLOOR)
    hat = total[:, :head]
    grad = scale * hat - scale * scale * scale * key * jnp.mean(key * hat, axis=1, keepdims=True)
    out_ref[:, :head] = grad.astype(BF)
    out_ref[:, head:] = total[:, head:].astype(BF)


def heads_sum(pieces, weights, columns):
    total = 0.0
    for piece, rows in zip(pieces, weights):
        term = lax.dot_general(
            piece, rows[:, columns[0] : columns[1]], CONTRACT_LAST, preferred_element_type=F32
        )
        total = total + term.astype(BF).astype(F32)
    return total.astype(BF)


def token_kernel(columns, *refs):
    far = jnp.concatenate([refs[3][...], refs[4][...]], axis=0)
    pieces = (refs[0][...], refs[1][...], refs[2][...], far)
    refs[9][...] = heads_sum(pieces, refs[5:9], columns)


def store_kernel(columns, *refs):
    weights, out_ref = refs[8:12], refs[12]
    for half in range(2):

        @pl.when(pl.program_id(0) == half)
        def _():
            pieces = tuple(ref[...] for ref in refs[4 * half : 4 * half + 4])
            out_ref[...] = heads_sum(pieces, weights, columns)


def ring4(value, axis):
    half = value.shape[0] // 2
    below = shift(value, axis, 1)
    above = shift(value, axis, -1)
    far_a = shift(below[:half], axis, 1)
    far_b = shift(above[half:], axis, -1)
    return value, above, below, far_a, far_b


def all4(value, axis):
    return value, shift(value, axis, -1), shift(value, axis, 1), shift(value, axis, 2)


def ring8(value, axis):
    half = value.shape[0] // 2
    below, above = [value], [value]
    for _ in range(3):
        below.append(shift(below[-1], axis, 1))
        above.append(shift(above[-1], axis, -1))
    far_a = shift(below[3][:half], axis, 1)
    far_b = shift(above[3][half:], axis, -1)
    return [value, above[1], above[2], above[3], far_a, below[3], below[2], below[1], far_b]


def swap(value):
    return lax.ppermute(value, "c", [(0, 1), (1, 0)])


def copy_for_each(shard, axis):
    copies = jnp.broadcast_to(shard, (lax.axis_size(axis), *shard.shape))
    return lax.all_to_all(copies, axis, split_axis=0, concat_axis=0, tiled=True)


def body(
    tokens,
    cotangent,
    mix_query,
    mix_key,
    mix_value,
    beta_pre,
    decay_pre,
    decay_rate,
    passages,
    passage_ids,
    query_weight,
    key_weight,
    value_weight,
    gate_weight,
):
    tok_rows = tokens.shape[0]
    width, head = query_weight.shape
    per_owner, rows_each = passages.shape[:2]
    blocks_n, per_block = passage_ids.shape
    span = tok_rows // blocks_n
    scale = SCORE_GAIN * head ** (-0.5)
    z, y, c, x = (lax.axis_index(a) for a in ("z", "y", "c", "x"))
    slice_w = width // 4

    pos = jnp.stack([z, y, c]).astype(jnp.int32)

    tok_pieces = all4(tokens, "x")

    flat_rows = passages.reshape(per_owner * rows_each, width)
    key_low = lax.optimization_barrier(
        jnp.dot(flat_rows, key_weight, preferred_element_type=F32).astype(BF)
    )
    value_all = jnp.dot(flat_rows, value_weight, preferred_element_type=F32).astype(BF)
    key_float = key_low.astype(F32)
    key_scale = lax.rsqrt(jnp.mean(key_float * key_float, axis=-1, keepdims=True) + NORM_FLOOR)
    key_hat = (key_float * key_scale).astype(BF)
    packed = jnp.concatenate([key_hat, value_all], axis=-1).reshape(per_owner, rows_each, 2 * head)
    kv_own = copy_for_each(packed[None], "y").reshape(4, *packed.shape)
    kv_other = swap(kv_own)

    query_acc = 0.0
    gate_acc = 0.0
    for n, piece in ((0, tok_pieces[0]), (1, tok_pieces[1]), (3, tok_pieces[2]), (2, tok_pieces[3])):
        first = ((x + n) & 3) * slice_w
        query_acc = query_acc + jnp.dot(
            piece,
            lax.dynamic_slice_in_dim(query_weight, first, slice_w, 0),
            preferred_element_type=F32,
        )
        gate_rows = lax.dynamic_slice_in_dim(gate_weight, first, slice_w, 1)
        gate_acc = gate_acc + jnp.sum(piece.astype(F32) * gate_rows.astype(F32), axis=1)
    query_low = lax.optimization_barrier(query_acc.astype(BF))
    query_float = query_low.astype(F32)
    query_scale = lax.rsqrt(
        jnp.mean(query_float * query_float, axis=-1, keepdims=True) + NORM_FLOOR
    )
    query_hat = (query_float * query_scale).astype(BF)
    gate_open = jax.nn.sigmoid(gate_acc)
    flat_ids = passage_ids.reshape(1, -1)
    digits = jnp.concatenate([flat_ids // 32, flat_ids % 32], axis=0).astype(BF)
    digits = jnp.pad(digits, ((0, 30), (0, 2 * head - digits.shape[1])))
    pieces = ring8(
        jnp.concatenate([jnp.concatenate([query_hat, cotangent], axis=1), digits], axis=0), "z"
    )

    gate_column = jnp.pad(
        jnp.broadcast_to(gate_weight.reshape(width, 1), (width, 2)), ((0, 0), (0, 126))
    )
    weights = jnp.concatenate([key_weight, value_weight, query_weight, gate_column], axis=1)
    weights, _ = lax.optimization_barrier((weights, tok_pieces[3]))
    weights = weights.reshape(4, slice_w, weights.shape[1])

    def weight_rows(step):
        rows = lax.dynamic_index_in_dim(weights, (x + step) & 3, 0, keepdims=False)
        return rows if step == 0 else shift(rows, "x", step)

    weights = [weight_rows(step) for step in (0, -1, 1, 2)]

    any_space = pl.BlockSpec(memory_space=pl.ANY)
    smem = pl.BlockSpec(memory_space=pltpu.SMEM)
    vmem = pl.BlockSpec(memory_space=pltpu.VMEM)
    stores = [
        pltpu.VMEM((8, *pieces[0].shape), BF),
        pltpu.VMEM((64, rows_each, 2 * head), BF),
    ]
    pieces = (*pieces, kv_own, kv_other)
    params = pltpu.CompilerParams(vmem_limit_bytes=60 * 1024 * 1024)
    message, codes, count = pl.pallas_call(
        functools.partial(sums_kernel, scale, blocks_n * per_block),
        out_shape=[
            jax.ShapeDtypeStruct((8, 9 * blocks_n, 2 * span), F32),
            jax.ShapeDtypeStruct((72,), jnp.int32),
            jax.ShapeDtypeStruct((1,), jnp.int32),
        ],
        in_specs=[smem, vmem] + [any_space] * 11,
        out_specs=[vmem, smem, smem],
        scratch_shapes=stores
        + [
            pltpu.VMEM((8, 128), jnp.int32),
            pltpu.SMEM((8, 128), jnp.int32),
            pltpu.SemaphoreType.DMA((10,)),
            pltpu.SemaphoreType.DMA((64,)),
        ],
        compiler_params=params,
        name="sums",
    )(pos, gate_open.reshape(blocks_n, span), *pieces)
    arrived = lax.all_to_all(message, "z", split_axis=0, concat_axis=0, tiled=True)

    def part_shape(owners):
        return jax.ShapeDtypeStruct((owners * per_owner, rows_each, 2 * head), BF)

    mine_far, mine_rest, other_far, other_rest, q_parts, totals = pl.pallas_call(
        functools.partial(terms_kernel, scale),
        out_shape=[
            part_shape(1),
            part_shape(3),
            part_shape(1),
            part_shape(3),
            jax.ShapeDtypeStruct((8, tok_rows, head), BF),
            jax.ShapeDtypeStruct((8 * blocks_n, 2 * span), F32),
        ],
        in_specs=[smem, smem, smem, vmem] + [any_space] * 11,
        out_specs=[any_space] * 4 + [vmem, vmem],
        scratch_shapes=stores
        + [
            pltpu.VMEM((8 * per_owner, rows_each, 2 * head), BF),
            pltpu.VMEM((8, tok_rows, head), F32),
            pltpu.VMEM((8 * blocks_n, 2 * span), F32),
            pltpu.SemaphoreType.DMA((9,)),
            pltpu.SemaphoreType.DMA((64,)),
        ],
        compiler_params=params,
        name="terms",
    )(codes, count, pos, arrived, *pieces)

    def plus(a, b):
        return (a.astype(F32) + b.astype(F32)).astype(BF)

    got_far = swap(other_far)
    got_rest = swap(other_rest)
    half = per_owner // 2
    got_a = shift(plus(mine_far[:half], got_far[:half]), "y", 1)
    got_b = shift(plus(mine_far[half:], got_far[half:]), "y", -1)
    near, back = 2 * per_owner, 0
    near_a, near_b, back_a, back_b = lax.optimization_barrier(
        tuple(
            plus(mine_rest[at : at + half], got_rest[at : at + half])
            for at in (near, near + half, back, back + half)
        )
    )
    early_b = shift(near_b, "y", 1)
    early_a = shift(back_a, "y", -1)
    late_a = shift(plus(near_a, got_a), "y", 1)
    late_b = shift(plus(back_b, got_b), "y", -1)

    q_back = lax.all_to_all(q_parts, "z", split_axis=0, concat_axis=0, tiled=True)
    qhat_grad = jnp.sum(q_back.astype(F32), axis=0)
    query_grad = (
        query_scale * qhat_grad
        - query_scale**3 * query_float * jnp.mean(query_float * qhat_grad, axis=-1, keepdims=True)
    ).astype(BF)
    mix_query, _ = lax.optimization_barrier((mix_query, q_parts))
    mixed_dot = mixer_dot(
        mix_query, mix_key, mix_value, cotangent, beta_pre, decay_pre, decay_rate
    ).reshape(tok_rows)
    own_totals = lax.dynamic_slice_in_dim(totals, z * blocks_n, blocks_n, 0)
    retrieved_dot = own_totals[:, span:].reshape(tok_rows)
    gate_grad = (retrieved_dot - mixed_dot) * gate_open * (1.0 - gate_open)
    high = gate_grad.astype(BF)
    rest = (gate_grad - high.astype(F32)).astype(BF)
    columns = jnp.pad(jnp.stack([high, rest], axis=1), ((0, 0), (0, 126)))
    token_pieces = ring4(jnp.concatenate([query_grad, columns], axis=1), "x")
    token_grad = pl.pallas_call(
        functools.partial(token_kernel, (2 * head, 3 * head + 128)),
        out_shape=jax.ShapeDtypeStruct((tok_rows, slice_w), BF),
        in_specs=[vmem] * 9,
        out_specs=vmem,
        compiler_params=params,
        name="token_rows",
    )(*token_pieces, *weights)

    half_rows = half * rows_each
    steps = 2
    tile = (half // steps, rows_each, 2 * head)
    tile_rows = half_rows // steps
    grads = []
    for n, one, two in ((0, early_a, late_a), (1, early_b, late_b)):
        own_part = pl.BlockSpec(tile, lambda i, n=n: (i + (2 + n) * steps, 0, 0))
        sent = pl.BlockSpec(tile, lambda i: (i, 0, 0))
        grads.append(
            pl.pallas_call(
                finish_kernel,
                grid=(steps,),
                out_shape=jax.ShapeDtypeStruct((half_rows, 2 * head), BF),
                in_specs=[
                    pl.BlockSpec((tile_rows, head), lambda i, n=n: (i + n * steps, 0)),
                    own_part,
                    own_part,
                    sent,
                    sent,
                ],
                out_specs=pl.BlockSpec((tile_rows, 2 * head), lambda i: (i, 0)),
                compiler_params=params,
            )(key_low, mine_rest, got_rest, one, two)
        )
    up_b = shift(grads[1], "x", -1)
    down_a = shift(grads[0], "x", 1)
    down_b, up_a = shift(grads[1], "x", 1), shift(grads[0], "x", -1)
    far_a, far_b = shift(down_a, "x", 1), shift(up_b, "x", -1)
    weight_b = lax.optimization_barrier(
        lax.dot_general(
            flat_rows[half_rows:], grads[1][:, :head], CONTRACT_FIRST, preferred_element_type=F32
        )
    )
    weight_term = (
        weight_b
        + lax.dot_general(
            flat_rows[:half_rows], grads[0][:, :head], CONTRACT_FIRST, preferred_element_type=F32
        )
    ).astype(BF)
    weight_term = weight_term.reshape(32, 2, width // 64, head)
    weight_other = swap(lax.dynamic_index_in_dim(weight_term, c ^ 1, 1, keepdims=False))
    weight_mine = plus(lax.dynamic_index_in_dim(weight_term, c, 1, keepdims=False), weight_other)
    weight_back = lax.all_to_all(weight_mine, ("z", "y"), split_axis=0, concat_axis=0, tiled=True)
    key_weight_grad = jnp.sum(weight_back.astype(F32), axis=0)
    passage_grad = pl.pallas_call(
        functools.partial(store_kernel, (0, 2 * head)),
        grid=(2,),
        out_shape=jax.ShapeDtypeStruct((per_owner * rows_each, slice_w), BF),
        in_specs=[pl.BlockSpec((half_rows, 2 * head), lambda i: (0, 0))] * 8
        + [pl.BlockSpec((slice_w, 2 * head), lambda i: (0, 0))] * 4,
        out_specs=pl.BlockSpec((half_rows, slice_w), lambda i: (i, 0)),
        compiler_params=params,
        name="store_rows",
    )(grads[0], up_a, down_a, far_a, grads[1], up_b, down_b, far_b, *weights).reshape(
        per_owner, rows_each, slice_w
    )
    return (token_grad, passage_grad, key_weight_grad)


def solution(mesh):
    torus = Mesh(mesh.devices.reshape(8, 4, 2, mesh.shape["tp"]), ("z", "y", "c", "x"))

    return jax.shard_map(
        body,
        mesh=torus,
        in_specs=(
            P(ST, "x"),
            P(ST, "x"),
            P(ST, "x"),
            P(ST, "x"),
            P(ST, "x"),
            P("x", ST),
            P("x", ST),
            P("x"),
            P(ST, None, None),
            P(ST, None),
            P(None, "x"),
            P(None, "x"),
            P(None, "x"),
            P("x", None),
        ),
        out_specs=(P(ST, "x"), P(ST, None, "x"), P(ST, "x")),
        check_vma=False,
    )
```
